32 devices in a mesh: st: 16 (over z, y, x), tp: 2 (over core).
Axes of the slice: x: 2, y: 2, z: 4, core: 2. Of those that a mesh axis runs over, the one named last changes fastest.
Arguments:
- tokens: bfloat16 [16384, 2048], P('st', 'tp'), may hold values from -6 to 6
- norm_gain: float32 [2048], replicated, may hold values from 0.1 to 1.9
- branch_outer: bfloat16 [2048, 2048], P(None, 'tp'), may hold values from -0.125 to 0.125
- branch_gate: bfloat16 [2048, 2048], P(None, 'tp'), may hold values from -0.125 to 0.125
- branch_input: bfloat16 [2048, 2048], P(None, 'tp'), may hold values from -0.125 to 0.125
- conv_taps: float32 [3, 2048], P(None, 'tp'), may hold values from -3.5 to 3.5
- query_weight: bfloat16 [2048, 1024], P(None, 'tp'), may hold values from -0.125 to 0.125
- query_gain: float32 [128], replicated, may hold values from 0.1 to 1.9
- head_scale: float32 [8], P('tp'), may hold values from 1 to 240
- store: bfloat16 [256, 64, 2048], P('st'), may hold values from -6 to 6
- store_gain: float32 [2048], replicated, may hold values from 0.1 to 1.9
- key_weight: bfloat16 [2048, 256], P(None, 'tp'), may hold values from -0.125 to 0.125
- value_weight: bfloat16 [2048, 256], P(None, 'tp'), may hold values from -0.125 to 0.125
- key_gain: float32 [128], replicated, may hold values from 0.1 to 1.9
- out_weight: bfloat16 [1024, 2048], P(None, 'tp'), may hold values from -0.1875 to 0.1875
- gate_logit: float32 [2048], P('tp'), may hold values from -1 to 4
- passage_ids: int32 [256, 4], P('st'), may hold values from 0 to 255, as said below
Outputs:
- mixed: bfloat16 [16384, 2048], P('st', 'tp')
The draws below stay inside these ranges and needn't reach their ends.
Inputs may be any that keep to these rules, and one draw needn't show every extreme that they name: `passage_ids`: passage p lies in the rows of store held by index p // 16 of st. Among the ids of the rows of one device (its 16 blocks), at most 4 name passages held by any one device, and exactly 4 name passages of some one device; each device names a passage of the device before it and one of the device half the axis away.
All inputs are finite; a program needn't handle non-finite values.
Results may differ from the reference program's by a relative error of at most 0.006.
The reference program's roundings to bfloat16 on the way count: a program that leaves them out, or rounds other values in their place, can miss the bound.
Values may be sent and summed in bfloat16 or wider, within the bound.
A program may use at most 128 MiB of HBM per device.

```python
import math
import jax
import jax.numpy as jnp
from jax import lax

D = 2048
HEADS = 8
KV_HEADS = 2
HEAD_DIM = 128
SEQ = 128
BLK = 64
PB = 4
PLEN = 64
TOK_DEV = 1024
PDEV = 16
TOKENS = 16384
PASSAGES = 256
N_ST = 16


def draw_head_scale(key, part):
    first_key = jax.random.fold_in(jax.random.fold_in(key, 29), 0)
    scales = jnp.exp(jax.random.uniform(first_key, (HEADS,), jnp.float32, math.log(1.0), math.log(4.0)))
    return scales.astype(jnp.float32)


def draw_passage_ids(key, part):
    requests = TOK_DEV // BLK * PB
    capacity = max(2, (requests + N_ST - 1) // N_ST)
    slots = N_ST * capacity

    def one_device(device):
        device_key = jax.random.fold_in(jax.random.fold_in(key, 17), device)
        keys_list = jax.random.split(device_key, 5)
        slot_order = jnp.arange(slots, dtype=jnp.int32)
        scores = jax.random.randint(keys_list[0], (slots,), 0, 1 << 20) * slots + slot_order
        owners = slot_order // capacity
        ranks = slot_order % capacity
        filled = jax.random.randint(keys_list[1], (), 0, N_ST)
        before = (device - 1) % N_ST
        across = (device + N_ST // 2) % N_ST
        forced = (owners == filled) | ((owners == before) | (owners == across)) & (ranks == 0)
        scores = jnp.where(forced, slot_order - slots, scores)
        picked = jnp.argsort(scores, stable=True)[:requests].astype(jnp.int32)
        chosen_owner = picked // capacity
        local_index = jnp.minimum(jax.random.randint(keys_list[2], (requests,), 0, PDEV), jax.random.randint(keys_list[3], (requests,), 0, PDEV))
        ids = chosen_owner * PDEV + local_index
        shuffle = jax.random.permutation(keys_list[4], requests)
        return ids[shuffle].reshape(requests // PB, PB)
    every = jax.vmap(one_device)(jnp.arange(N_ST, dtype=jnp.int32))
    return every.reshape(N_ST * (TOK_DEV // BLK), PB).astype(jnp.int32)


def level_of(stream_key, extent, cuts, low, largest):
    def one(axis_at, blocks):
        heights = jax.random.uniform(jax.random.fold_in(jax.random.fold_in(stream_key, 6), axis_at), (blocks,), jnp.float32, low / len(cuts), largest / len(cuts))
        return jnp.repeat(jnp.exp(heights), extent[axis_at] // blocks).reshape((-1,) + (1,) * (len(extent) - axis_at - 1))

    level = one(*cuts[0])
    for cut in cuts[1:]:
        level = level * one(*cut)
    return level


def gaussian(key, extent, width, bound, shards=(), kind=jnp.bfloat16):
    loudness = level_of(key, extent, shards, -0.22, 0.18) if shards else 1.0
    array = jax.random.normal(key, extent, jnp.float32) * width * loudness
    return jnp.minimum(jnp.maximum(array, -bound), bound).astype(kind)


def setup_inputs(seed: int = 0) -> dict:
    splits = jax.random.split(jax.random.key(seed), 18)
    tokens = gaussian(splits[0], (TOKENS, D), 1.0, 6.0, ((0, 16), (1, 2)))
    norm_gain = jnp.clip(1.0 + 0.18 * jax.random.normal(splits[1], (D,), jnp.float32), 0.1, 1.9)
    branch_outer = gaussian(splits[2], (D, D), D ** -0.5, 0.125, ((1, 2),))
    branch_gate = gaussian(splits[3], (D, D), D ** -0.5, 0.125, ((1, 2),))
    branch_input = gaussian(splits[4], (D, D), D ** -0.5, 0.125, ((1, 2),))
    conv_taps = gaussian(splits[5], (3, D), 3 ** -0.5, 3.5, ((1, 2),), jnp.float32)
    query_weight = gaussian(splits[6], (D, HEADS * HEAD_DIM), D ** -0.5, 0.125, ((1, 2),))
    query_gain = jnp.clip(1.0 + 0.18 * jax.random.normal(splits[7], (HEAD_DIM,), jnp.float32), 0.1, 1.9)
    head_scale = draw_head_scale(jax.random.fold_in(splits[17], 71), 0)
    store = gaussian(splits[9], (PASSAGES, PLEN, D), 1.0, 6.0, ((0, 16),))
    store_gain = jnp.clip(1.0 + 0.18 * jax.random.normal(splits[10], (D,), jnp.float32), 0.1, 1.9)
    key_weight = gaussian(splits[11], (D, KV_HEADS * HEAD_DIM), D ** -0.5, 0.125, ((1, 2),))
    value_weight = gaussian(splits[12], (D, KV_HEADS * HEAD_DIM), D ** -0.5, 0.125, ((1, 2),))
    key_gain = jnp.clip(1.0 + 0.18 * jax.random.normal(splits[13], (HEAD_DIM,), jnp.float32), 0.1, 1.9)
    out_weight = gaussian(splits[14], (HEADS * HEAD_DIM, D), (HEADS * HEAD_DIM) ** -0.5, 0.1875, ((1, 2),))
    gate_logit = jnp.clip(-1.0 + 5.0 * jax.random.uniform(splits[15], (D,), jnp.float32) ** level_of(splits[15], (D,), ((0, 2),), -0.2, 0.2), -1.0, 4.0)
    passage_ids = draw_passage_ids(jax.random.fold_in(splits[17], 71), 0)
    return dict(tokens=tokens, norm_gain=norm_gain, branch_outer=branch_outer, branch_gate=branch_gate, branch_input=branch_input, conv_taps=conv_taps, query_weight=query_weight, query_gain=query_gain, head_scale=head_scale, store=store, store_gain=store_gain, key_weight=key_weight, value_weight=value_weight, key_gain=key_gain, out_weight=out_weight, gate_logit=gate_logit, passage_ids=passage_ids)


EPS = 1e-06

def norm_rows(values, gain):
    values = values.astype(jnp.float32)
    return values * lax.rsqrt(lax.optimization_barrier(jnp.mean(values * values, axis=-1, keepdims=True)) + EPS) * gain.astype(jnp.float32)

def causal_taps(product, conv_taps):
    token_rows, model_width = product.shape
    grouped = product.reshape(token_rows // SEQ, SEQ, model_width)
    padded = jnp.pad(grouped, ((0, 0), (2, 0), (0, 0)))
    summed = padded[:, 0:SEQ] * conv_taps[0] + padded[:, 1:SEQ + 1] * conv_taps[1] + padded[:, 2:SEQ + 2] * conv_taps[2]
    return summed.reshape(token_rows, model_width)

def passage_partials(queries, key_rows, value_rows):
    scores = jnp.einsum('nqgrd,nkgd->ngrqk', queries.astype(jnp.float32), key_rows.astype(jnp.float32))
    maxima = lax.optimization_barrier(jnp.max(scores, axis=-1))
    weights = jnp.exp(scores - maxima[..., None])
    totals = lax.optimization_barrier(jnp.sum(weights, axis=-1))
    shares = (weights / totals[..., None]).astype(jnp.bfloat16)
    partial_value = jnp.einsum('ngrqk,nkgd->nqgrd', shares.astype(jnp.float32), value_rows.astype(jnp.float32)).astype(jnp.bfloat16)
    return (partial_value, maxima, totals)

def combine_passages(partial_value, maxima, totals):
    highest = lax.optimization_barrier(jnp.max(maxima, axis=1, keepdims=True))
    weight = jnp.exp(maxima - highest) * totals
    denominator = lax.optimization_barrier(jnp.sum(weight, axis=1))
    weight = jnp.transpose(weight, (0, 1, 4, 2, 3))
    summed = lax.optimization_barrier(jnp.sum(partial_value.astype(jnp.float32) * weight[..., None], axis=1))
    return summed / jnp.transpose(denominator, (0, 3, 1, 2))[..., None]

def reference(tokens, norm_gain, branch_outer, branch_gate, branch_input, conv_taps, query_weight, query_gain, head_scale, store, store_gain, key_weight, value_weight, key_gain, out_weight, gate_logit, passage_ids):
    normed = norm_rows(tokens, norm_gain).astype(jnp.bfloat16)
    gate_outer = jnp.dot(normed, branch_outer, preferred_element_type=jnp.float32)
    gate_inner = jnp.dot(normed, branch_gate, preferred_element_type=jnp.float32)
    conv_input = jnp.dot(normed, branch_input, preferred_element_type=jnp.float32)
    conv_out = gate_outer * causal_taps(gate_inner * conv_input, conv_taps.astype(jnp.float32))
    token_rows = tokens.shape[0]
    repeat = HEADS // KV_HEADS
    raw_query = jnp.dot(normed, query_weight, preferred_element_type=jnp.float32).reshape(token_rows, HEADS, HEAD_DIM)
    queries = (norm_rows(raw_query, query_gain) * (head_scale[:, None] / math.sqrt(HEAD_DIM))).astype(jnp.bfloat16)
    queries = queries.reshape(token_rows // BLK, BLK, KV_HEADS, repeat, HEAD_DIM)
    memory = norm_rows(store.reshape(PASSAGES * PLEN, D), store_gain).astype(jnp.bfloat16)
    raw_key = jnp.dot(memory, key_weight, preferred_element_type=jnp.float32).reshape(PASSAGES * PLEN, KV_HEADS, HEAD_DIM)
    key_rows = norm_rows(raw_key, key_gain).astype(jnp.bfloat16).reshape(PASSAGES, PLEN, KV_HEADS, HEAD_DIM)
    value_rows = jnp.dot(memory, value_weight, preferred_element_type=jnp.float32).astype(jnp.bfloat16)
    value_rows = value_rows.reshape(PASSAGES, PLEN, KV_HEADS, HEAD_DIM)

    def one_block(pieces):
        block_query, chosen = pieces
        asked_query = jnp.broadcast_to(block_query[None], (PB,) + block_query.shape)
        return passage_partials(asked_query, key_rows[chosen], value_rows[chosen])
    partial_value, maxima, totals = lax.map(one_block, (queries, passage_ids))
    attended = combine_passages(partial_value, maxima, totals).astype(jnp.bfloat16).reshape(token_rows, HEADS * HEAD_DIM)
    cross = jnp.dot(attended, out_weight, preferred_element_type=jnp.float32)
    return (conv_out + jax.nn.sigmoid(gate_logit) * cross).astype(jnp.bfloat16)
```

```python
import functools
import math

import jax
import jax.numpy as jnp
from jax import lax
from jax.experimental import pallas as pl
from jax.experimental.pallas import tpu as pltpu
from jax.sharding import PartitionSpec as P

MESH = pl.DeviceIdType.MESH
LANES = 128
SEQ = 128
EPS = 1e-06
NT = (((1,), (1,)), ((), ()))
TN = (((0,), (0,)), ((), ()))


def norm_rows(values, gain):
    values = values.astype(jnp.float32)
    return values * lax.rsqrt(jnp.mean(values * values, axis=-1, keepdims=True) + EPS) * gain


def largest(total, options):
    return next(c for c in options if total % c == 0)


def layer_kernel(
    cfg, slots, blocks, head_scale, pick_hbm, tokens_hbm, norm_gain_hbm, outer_hbm, gate_hbm,
    input_hbm, taps_hbm, query_hbm, query_gain_hbm, store_hbm, store_gain_hbm, key_hbm, value_hbm,
    key_gain_hbm,
    attended_hbm, conv_hbm,
    half, normed, outer, gate, inp, query, pair, held, table, mirror_table, send_buf, relay_buf,
    received, q, partials, stats, attended, conv, norm_gain, taps, query_gain, store_gain, key_gain,
    pick_row, picks, wanted,
    store_sem, side_sem, weight_sem, swap_sem, id_send, id_recv, mirror_send, mirror_recv,
    send_sem, relay_sem, recv_sem, conv_sem, part_send, part_recv, out_sem,
):
    n, planes, capacity, per_block, groups, repeat, head_dim, block_rows, relay_after = cfg
    me = lax.axis_index("st")
    core = lax.axis_index("tp")
    plane = n // planes
    level, place = me // plane, lax.rem(me, plane)
    relays = planes == 4
    middle = (level == 1) | (level == 2)
    mirror = (planes - 1 - level) * plane + place
    levels = [level]
    if relays:
        levels = [
            level,
            level + 1 - 2 * lax.rem(level, 2),
            level + 2 - 4 * lax.rem(level // 2, 2),
            3 - level,
        ]
    near = (0, 1) if relays else (0,)
    far = (2, 3) if relays else ()

    def peer(step, j):
        return levels[step] * plane + lax.rem(place + j, plane)

    def every(body, steps=near + far, own=False):
        for step in steps:

            def run(j, carry, step=step):
                body(step, j)
                return carry

            lax.fori_loop(1 if step == 0 and not own else 0, plane, run, 0)

    chunks, chunk_rows = held.shape[0], held.shape[1]
    passage_rows = table.shape[1]
    chunk_passages = chunk_rows // passage_rows
    key_width = key_hbm.shape[1]
    token_rows = tokens_hbm.shape[0]

    def load(c):
        return pltpu.make_async_copy(
            store_hbm.at[pl.ds(c * chunk_rows, chunk_rows)], held.at[c], store_sem.at[c]
        )

    sides = [
        pltpu.make_async_copy(source, target, side_sem.at[k])
        for k, (source, target) in enumerate(
            [
                (store_gain_hbm, store_gain),
                (key_hbm, pair.at[:, pl.ds(0, key_width)]),
                (value_hbm, pair.at[:, pl.ds(key_width, value_hbm.shape[1])]),
                (key_gain_hbm, key_gain),
                (pick_hbm, pick_row),
                (pick_hbm, picks.at[me]),
                (norm_gain_hbm, norm_gain),
                (query_gain_hbm, query_gain),
                (taps_hbm, taps),
                (tokens_hbm, half.at[core]),
            ]
        )
    ]
    weights = [
        pltpu.make_async_copy(source, target, weight_sem.at[k])
        for k, (source, target) in enumerate(
            [(query_hbm, query), (gate_hbm, gate), (input_hbm, inp), (outer_hbm, outer)]
        )
    ]

    def remote(source, target, sent, got, to):
        return pltpu.make_async_remote_copy(
            src_ref=source,
            dst_ref=target,
            send_sem=sent,
            recv_sem=got,
            device_id=to,
            device_id_type=MESH,
        )

    across = {"tp": 1 - core}
    swap_tokens = remote(tokens_hbm, half.at[core], swap_sem.at[0], swap_sem.at[1], across)

    def send_ids(step, j):
        to = peer(step, j)
        return remote(pick_row, picks.at[me], id_send.at[to], id_recv.at[me], {"st": to})

    def take_ids(step, j):
        owner = peer(step, j)
        return remote(pick_row, picks.at[owner], id_send.at[owner], id_recv.at[owner], {"st": owner})

    def swap_table(c):
        at = pl.ds(c * chunk_passages, chunk_passages)
        return remote(
            table.at[at], mirror_table.at[at], mirror_send.at[c], mirror_recv.at[c], {"st": mirror}
        )

    def wants(to, owner):
        return [wanted[to, 0, owner * capacity + r] for r in range(capacity)]

    def fill(step, j):
        to = peer(step, j)
        for r, pick in enumerate(wants(to, me)):
            send_buf[to * capacity + r] = table[pick]

    def send(step, j):
        to = peer(step, j)
        return remote(
            send_buf.at[pl.ds(to * capacity, capacity)],
            received.at[pl.ds(me * capacity, capacity)],
            send_sem.at[to],
            recv_sem.at[me],
            {"st": to},
        )

    def take(step, j):
        owner = peer(step, j)
        return remote(
            send_buf.at[pl.ds(owner * capacity, capacity)],
            received.at[pl.ds(owner * capacity, capacity)],
            send_sem.at[owner],
            recv_sem.at[owner],
            {"st": owner},
        )

    def fill_relay(step, j):
        at = (step * plane + j) * capacity
        for r, pick in enumerate(wants(peer(step, j), mirror)):
            relay_buf[at + r] = mirror_table[pick]

    def relay(step, j):
        k = step * plane + j
        return remote(
            relay_buf.at[pl.ds(k * capacity, capacity)],
            received.at[pl.ds(mirror * capacity, capacity)],
            relay_sem.at[k],
            recv_sem.at[mirror],
            {"st": peer(step, j)},
        )

    def project(c):
        load(c).wait()
        memory = norm_rows(held[c], store_gain[...]).astype(jnp.bfloat16)
        raw = jnp.dot(memory, pair[...], preferred_element_type=jnp.float32)
        keys = [
            norm_rows(raw[:, g * head_dim : (g + 1) * head_dim], key_gain[...])
            for g in range(groups)
        ]
        done = jnp.concatenate(keys + [raw[:, groups * head_dim :]], axis=1).astype(jnp.bfloat16)
        table[pl.ds(c * chunk_passages, chunk_passages)] = done.reshape(
            chunk_passages, passage_rows, done.shape[1]
        )

    load(0).start()
    for side in sides[:-1]:
        side.start()
    for c in range(1, chunks):
        load(c).start()
    barrier = pltpu.get_barrier_semaphore()

    def greet(step, j):
        pl.semaphore_signal(barrier, inc=1, device_id={"st": peer(step, j)}, device_id_type=MESH)

    every(greet)
    pl.semaphore_signal(barrier, inc=1, device_id=across, device_id_type=MESH)
    for k in range(4):
        sides[k].wait()
    for c in range(chunks):
        project(c)
        if c == 0:
            sides[4].wait()
            pl.semaphore_wait(barrier, n)
            every(lambda step, j: send_ids(step, j).start())
            sides[-1].start()
            swap_tokens.start()
        if relays and c > 0:

            @pl.when(middle)
            def _(c=c):
                swap_table(c - 1).start()

    for weight in weights:
        weight.start()
    if relays:

        @pl.when(middle)
        def _():
            swap_table(chunks - 1).start()

    for side in sides[5:-1]:
        side.wait()
    every(lambda step, j: take_ids(step, j).wait_recv())
    listed = pltpu.make_async_copy(picks, wanted, side_sem.at[len(sides)])
    listed.start()
    listed.wait()
    every(fill, near)
    if relays:

        @pl.when(jnp.logical_not(middle))
        def _():
            every(fill, far)

    every(lambda step, j: send(step, j).start(), near)
    if relays:

        @pl.when(jnp.logical_not(middle))
        def _():
            every(lambda step, j: send(step, j).start(), far)

    for r, pick in enumerate(wants(me, me)):
        received[me * capacity + r] = table[pick]

    sides[-1].wait()
    swap_tokens.wait()
    norm_tile = largest(token_rows, (128, 64, 32, 16, 8))

    def normalize(i, carry):
        rows = pl.ds(pl.multiple_of(i * norm_tile, norm_tile), norm_tile)
        whole = jnp.concatenate([half[0, rows, :], half[1, rows, :]], axis=1)
        normed[rows, :] = norm_rows(whole, norm_gain[...]).astype(jnp.bfloat16)
        return carry

    lax.fori_loop(0, token_rows // norm_tile, normalize, 0)

    weights[0].wait()
    tile_blocks = largest(token_rows // block_rows, (4, 2, 1))
    tile_rows = tile_blocks * block_rows

    def ask(i, carry):
        rows = pl.ds(pl.multiple_of(i * tile_rows, tile_rows), tile_rows)
        raw = jnp.dot(normed[rows, :], query[...], preferred_element_type=jnp.float32)
        for g in range(groups):
            for h in range(repeat):
                at = (g * repeat + h) * head_dim
                scale = head_scale[g * repeat + h] * (1.0 / math.sqrt(head_dim))
                head = norm_rows(raw[:, at : at + head_dim], query_gain[...]) * scale
                head = head.astype(jnp.bfloat16)
                for b in range(tile_blocks):
                    q[(i * tile_blocks + b) * groups + g, pl.ds(h * block_rows, block_rows), :] = (
                        head[b * block_rows : (b + 1) * block_rows]
                    )
        return carry

    lax.fori_loop(0, token_rows // tile_rows, ask, 0)

    for weight in weights[1:]:
        weight.wait()
    conv_rows = largest(token_rows // SEQ, (4, 2, 1)) * SEQ
    conv_columns = largest(conv.shape[1] // LANES, (2, 1)) * LANES
    across_tiles = conv.shape[1] // conv_columns
    down_tiles = token_rows // conv_rows
    conv_tiles = across_tiles * down_tiles

    def conv_out(t):
        c, i = t // down_tiles, lax.rem(t, down_tiles)
        rows = pl.ds(pl.multiple_of(i * conv_rows, conv_rows), conv_rows)
        columns = pl.ds(pl.multiple_of(c * conv_columns, conv_columns), conv_columns)
        return pltpu.make_async_copy(
            conv.at[rows, columns], conv_hbm.at[rows, columns], conv_sem.at[t]
        )

    def branch(t, carry):
        c, i = t // down_tiles, lax.rem(t, down_tiles)
        rows = pl.ds(pl.multiple_of(i * conv_rows, conv_rows), conv_rows)
        columns = pl.ds(pl.multiple_of(c * conv_columns, conv_columns), conv_columns)
        left = normed[rows, :]
        z = jnp.dot(left, gate[:, columns], preferred_element_type=jnp.float32)
        z = z * jnp.dot(left, inp[:, columns], preferred_element_type=jnp.float32)
        at = lax.rem(lax.broadcasted_iota(jnp.int32, (conv_rows, 1), 0), SEQ)
        one = jnp.where(at < 1, 0.0, pltpu.roll(z, 1, 0))
        two = jnp.where(at < 2, 0.0, pltpu.roll(z, 2, 0))
        summed = (
            two * taps[0:1, columns] + one * taps[1:2, columns] + z * taps[2:3, columns]
        )
        conv[rows, columns] = (
            jnp.dot(left, outer[:, columns], preferred_element_type=jnp.float32) * summed
        )
        conv_out(t).start()
        return carry

    before = min(conv_tiles, relay_after) if relays else conv_tiles
    lax.fori_loop(0, before, branch, 0)
    if relays:

        @pl.when(middle)
        def _():
            for c in range(chunks):
                swap_table(c).wait()
            every(fill_relay, near, own=False)
            every(lambda step, j: relay(step, j).start(), near)
            for r, pick in enumerate(wants(me, mirror)):
                received[mirror * capacity + r] = mirror_table[pick]

        lax.fori_loop(before, conv_tiles, branch, 0)

    width = repeat * block_rows

    def attend(step, j):
        owner = peer(step, j)
        if step == 0:

            @pl.when(j > 0)
            def _():
                take(step, j).wait_recv()
        elif step == 3:

            @pl.when(jnp.logical_not(middle & (j == 0)))
            def _():
                take(step, j).wait_recv()
        else:
            take(step, j).wait_recv()
        for r in range(capacity):
            slot = owner * capacity + r
            block = blocks[slot]
            for g in range(groups):
                passage = received[slot]
                asked = q[block * groups + g]
                key = passage[:, g * head_dim : (g + 1) * head_dim]
                value = passage[:, (groups + g) * head_dim : (groups + g + 1) * head_dim]
                scores = lax.dot_general(key, asked, NT, preferred_element_type=jnp.float32)
                top = jnp.max(scores, axis=0, keepdims=True)
                weight = jnp.exp(scores - top)
                total = jnp.sum(weight, axis=0, keepdims=True)
                shares = (weight * (1.0 / total)).astype(jnp.bfloat16)
                part = lax.dot_general(value, shares, TN, preferred_element_type=jnp.float32)
                partials[slot * groups + g] = part.astype(jnp.bfloat16)
                stats[slot * groups + g, 0:1, :] = top
                stats[slot * groups + g, 1:2, :] = total

    every(attend, own=True)

    block_count = token_rows // block_rows
    parts = part_send.shape[0]
    part_blocks = block_count // parts
    part_rows = part_blocks * block_rows

    def swap_part(k):
        here = attended.at[core, pl.ds(k * part_rows, part_rows)]
        return remote(here, here, part_send.at[k], part_recv.at[k], across)

    def combine(b, carry):
        for g in range(groups):
            at = [slots[b * per_block + p] * groups + g for p in range(per_block)]
            tops = [stats[s, 0:1, :] for s in at]
            highest = functools.reduce(jnp.maximum, tops)
            scales = [jnp.exp(top - highest) * stats[s, 1:2, :] for top, s in zip(tops, at)]
            denominator = functools.reduce(jnp.add, scales)
            summed = functools.reduce(
                jnp.add, [partials[s].astype(jnp.float32) * scale for s, scale in zip(at, scales)]
            )
            done = jnp.transpose(summed * (1.0 / denominator)).astype(jnp.bfloat16)
            rows = pl.ds(pl.multiple_of(b * block_rows, block_rows), block_rows)
            for h in range(repeat):
                columns = slice((g * repeat + h) * head_dim, (g * repeat + h + 1) * head_dim)
                attended[core, rows, columns] = done[h * block_rows : (h + 1) * block_rows]
        return carry

    for k in range(parts):
        lax.fori_loop(k * part_blocks, (k + 1) * part_blocks, combine, 0)
        if k > 0:
            swap_part(k - 1).start()
    swap_part(parts - 1).start()

    def leave(index, side):
        wide = attended.shape[2]
        return pltpu.make_async_copy(
            attended.at[side],
            attended_hbm.at[:, pl.ds(pl.multiple_of(side * wide, LANES), wide)],
            out_sem.at[index],
        )

    leave(0, core).start()
    every(lambda step, j: send_ids(step, j).wait_send())
    every(lambda step, j: send(step, j).wait_send(), near)
    if relays:

        @pl.when(middle)
        def _():
            every(lambda step, j: relay(step, j).wait_send(), near)

        @pl.when(jnp.logical_not(middle))
        def _():
            every(lambda step, j: send(step, j).wait_send(), far)

    def landed(t, carry):
        conv_out(t).wait()
        return carry

    lax.fori_loop(0, conv_tiles, landed, 0)
    for k in range(parts):
        swap_part(k).wait()
    leave(1, 1 - core).start()
    leave(0, core).wait()
    leave(1, 1 - core).wait()


def on_device(
    planes,
    tokens,
    norm_gain,
    branch_outer,
    branch_gate,
    branch_input,
    conv_taps,
    query_weight,
    query_gain,
    head_scale,
    store,
    store_gain,
    key_weight,
    value_weight,
    key_gain,
    out_weight,
    gate_logit,
    passage_ids,
):
    n = lax.axis_size("st")
    token_rows, local_width = tokens.shape
    head_dim = query_gain.shape[0]
    local_heads = query_weight.shape[1] // head_dim
    groups = key_weight.shape[1] // head_dim
    repeat = local_heads // groups
    block_count, per_block = passage_ids.shape
    block_rows = token_rows // block_count
    passages, passage_rows, width = store.shape
    channels = branch_outer.shape[1]
    requests = block_count * per_block
    capacity = max(2, (requests + n - 1) // n)
    count = n * capacity
    flat = passage_ids.reshape(requests)
    owners = flat // passages
    order = jnp.arange(requests, dtype=jnp.int32)
    earlier = (owners[:, None] == owners[None, :]) & (order[None, :] < order[:, None])
    slots = owners * capacity + jnp.sum(earlier.astype(jnp.int32), axis=1)
    lanes = LANES * ((count + LANES - 1) // LANES)
    filled = slots[None, :] == jnp.arange(lanes, dtype=jnp.int32)[:, None]
    pick = jnp.sum(jnp.where(filled, (flat - owners * passages)[None], 0), axis=1)
    blocks = jnp.sum(jnp.where(filled, (order // per_block)[None], 0), axis=1)

    rows = passages * passage_rows
    chunks = largest(passages, (4, 2, 1))
    parts = largest(block_count, (4, 2, 1))
    pair_width = key_weight.shape[1] + value_weight.shape[1]
    wide = repeat * block_rows
    conv_tiles = (token_rows // (largest(token_rows // SEQ, (4, 2, 1)) * SEQ)) * (
        channels // (largest(channels // LANES, (2, 1)) * LANES)
    )
    plane = n // planes
    relays = planes == 4
    bf16, f32 = jnp.bfloat16, jnp.float32
    dma = pltpu.SemaphoreType.DMA
    smem = pl.BlockSpec(memory_space=pltpu.SMEM)
    anywhere = pl.BlockSpec(memory_space=pl.ANY)
    cfg = (n, planes, capacity, per_block, groups, repeat, head_dim, block_rows, RELAY_AFTER)
    attended, conv = pl.pallas_call(
        functools.partial(layer_kernel, cfg),
        out_shape=(
            jax.ShapeDtypeStruct((token_rows, 2 * local_heads * head_dim), bf16),
            jax.ShapeDtypeStruct((token_rows, channels), f32),
        ),
        in_specs=[smem] * 3 + [anywhere] * 14,
        out_specs=(anywhere, anywhere),
        scratch_shapes=[
            pltpu.VMEM((2, token_rows, local_width), bf16),
            pltpu.VMEM((token_rows, width), bf16),
            pltpu.VMEM((width, channels), bf16),
            pltpu.VMEM((width, channels), bf16),
            pltpu.VMEM((width, channels), bf16),
            pltpu.VMEM(query_weight.shape, bf16),
            pltpu.VMEM((width, pair_width), bf16),
            pltpu.VMEM((chunks, rows // chunks, width), bf16),
            pltpu.VMEM((passages, passage_rows, pair_width), bf16),
            pltpu.VMEM((passages, passage_rows, pair_width), bf16),
            pltpu.VMEM((count, passage_rows, pair_width), bf16),
            pltpu.VMEM((2 * plane * capacity if relays else 1, passage_rows, pair_width), bf16),
            pltpu.VMEM((count, passage_rows, pair_width), bf16),
            pltpu.VMEM((block_count * groups, wide, head_dim), bf16),
            pltpu.VMEM((count * groups, head_dim, wide), bf16),
            pltpu.VMEM((count * groups, 2, wide), f32),
            pltpu.VMEM((2, token_rows, local_heads * head_dim), bf16),
            pltpu.VMEM((token_rows, channels), f32),
            pltpu.VMEM((1, width), f32),
            pltpu.VMEM(conv_taps.shape, f32),
            pltpu.VMEM((1, head_dim), f32),
            pltpu.VMEM((1, width), f32),
            pltpu.VMEM((1, head_dim), f32),
            pltpu.VMEM((1, lanes), jnp.int32),
            pltpu.VMEM((n, 1, lanes), jnp.int32),
            pltpu.SMEM((n, 1, lanes), jnp.int32),
            dma((chunks,)),
            dma((11,)),
            dma((4,)),
            dma((2,)),
            dma((n,)),
            dma((n,)),
            dma((chunks,)),
            dma((chunks,)),
            dma((n,)),
            dma((2 * plane,)),
            dma((n,)),
            dma((conv_tiles,)),
            dma((parts,)),
            dma((parts,)),
            dma((2,)),
        ],
        compiler_params=pltpu.CompilerParams(
            collective_id=0, has_side_effects=True, vmem_limit_bytes=62 * 1024 * 1024
        ),
        cost_estimate=pl.CostEstimate(
            flops=2 * token_rows * width * (3 * channels + local_heads * head_dim),
            bytes_accessed=8 * width * channels,
            transcendentals=0,
        ),
        name="layer",
    )(
        slots,
        blocks,
        head_scale,
        pick[None],
        tokens,
        norm_gain[None],
        branch_outer,
        branch_gate,
        branch_input,
        conv_taps,
        query_weight,
        query_gain[None],
        store.reshape(rows, width),
        store_gain[None],
        key_weight,
        value_weight,
        key_gain[None],
    )
    cross = jnp.dot(attended, out_weight, preferred_element_type=jnp.float32)
    mixed = conv + jax.nn.sigmoid(gate_logit) * cross
    return mixed.astype(jnp.bfloat16)


RELAY_AFTER = 4


def planes_of(mesh):
    line = mesh.devices.reshape(mesh.shape["st"], -1)[:, 0]
    heights = [getattr(d, "coords", (0, 0, 0))[2] for d in line]
    planes = len(set(heights))
    plane = len(heights) // planes
    ordered = heights == [h for h in sorted(set(heights)) for _ in range(plane)]
    return planes if planes == 4 and ordered else 1


def solution(mesh):
    return jax.shard_map(
        functools.partial(on_device, planes_of(mesh)),
        mesh=mesh,
        in_specs=(
            P("st", "tp"),
            P(),
            P(None, "tp"),
            P(None, "tp"),
            P(None, "tp"),
            P(None, "tp"),
            P(None, "tp"),
            P(),
            P("tp"),
            P("st", None, None),
            P(),
            P(None, "tp"),
            P(None, "tp"),
            P(),
            P(None, "tp"),
            P("tp"),
            P("st", None),
        ),
        out_specs=P("st", "tp"),
        check_vma=False,
    )
```

```python
import functools
import math

import jax
import jax.numpy as jnp
from jax import lax
from jax.experimental import pallas as pl
from jax.experimental.pallas import tpu as pltpu
from jax.sharding import PartitionSpec as P

MESH = pl.DeviceIdType.MESH
LANES = 128
SEQ = 128
EPS = 1e-06
NN = (((1,), (0,)), ((), ()))
TN = (((0,), (0,)), ((), ()))


def norm_rows(values, gain):
    values = values.astype(jnp.float32)
    return values * lax.rsqrt(jnp.mean(values * values, axis=-1, keepdims=True) + EPS) * gain


def largest(total, options):
    return next(c for c in options if total % c == 0)


def layer_kernel(
    cfg, slots, blocks, head_scale, pick_hbm, tokens_hbm, norm_gain_hbm, outer_hbm, gate_hbm,
    input_hbm, taps_hbm, query_hbm, query_gain_hbm, store_hbm, store_gain_hbm, key_hbm, value_hbm,
    key_gain_hbm, out_weight_hbm, gate_logit_hbm,
    mixed_hbm,
    half, normed, outer, gate, inp, query, out_weight, pair, held, own_table, side_table, next_table,
    send_buf, received, q, partials, stats, attended, conv, norm_gain, taps, query_gain, store_gain, key_gain,
    gate_logit, pick_row, picks, wanted,
    store_sem, side_sem, weight_sem, swap_sem, id_send, id_recv, table_send, table_recv,
    send_sem, recv_sem, part_send, part_recv, out_sem,
):
    n, planes, capacity, per_block, groups, repeat, head_dim, block_rows = cfg
    me = lax.axis_index("st")
    core = lax.axis_index("tp")
    plane = n // planes
    level, place = me // plane, lax.rem(me, plane)
    relays = planes == 4
    middle = (level == 1) | (level == 2)
    edge = jnp.logical_not(middle)
    levels = [level]
    if relays:
        half_up = level // 2
        levels += [level + 1 - 2 * lax.rem(level, 2), 2 - half_up, 3 - 3 * half_up]
    beside = [at * plane + place for at in levels]

    def peer(step, j):
        return levels[step] * plane + lax.rem(place + j, plane)

    def every(body, steps, own=False):
        for step in steps:

            def run(j, carry, step=step):
                body(step, j)
                return carry

            lax.fori_loop(1 if step == 0 and not own else 0, plane, run, 0)

    steps = tuple(range(len(levels)))
    tables = [own_table, side_table, next_table]

    chunks, chunk_rows = held.shape[0], held.shape[1]
    passage_rows = own_table.shape[1]
    chunk_passages = chunk_rows // passage_rows
    key_width = key_hbm.shape[1]
    token_rows = tokens_hbm.shape[0]

    def load(c):
        return pltpu.make_async_copy(
            store_hbm.at[pl.ds(c * chunk_rows, chunk_rows)], held.at[c], store_sem.at[c]
        )

    sides = [
        pltpu.make_async_copy(source, target, side_sem.at[k])
        for k, (source, target) in enumerate(
            [
                (store_gain_hbm, store_gain),
                (key_hbm, pair.at[:, pl.ds(0, key_width)]),
                (value_hbm, pair.at[:, pl.ds(key_width, value_hbm.shape[1])]),
                (key_gain_hbm, key_gain),
                (pick_hbm, pick_row),
                (pick_hbm, picks.at[me]),
                (norm_gain_hbm, norm_gain),
                (query_gain_hbm, query_gain),
                (taps_hbm, taps),
                (gate_logit_hbm, gate_logit),
                (tokens_hbm, half.at[core]),
            ]
        )
    ]
    weights = [
        pltpu.make_async_copy(source, target, weight_sem.at[k])
        for k, (source, target) in enumerate(
            [
                (query_hbm, query),
                (gate_hbm, gate),
                (input_hbm, inp),
                (outer_hbm, outer),
                (out_weight_hbm, out_weight),
            ]
        )
    ]

    def remote(source, target, sent, got, to):
        return pltpu.make_async_remote_copy(
            src_ref=source,
            dst_ref=target,
            send_sem=sent,
            recv_sem=got,
            device_id=to,
            device_id_type=MESH,
        )

    across = {"tp": 1 - core}
    swap_tokens = remote(tokens_hbm, half.at[core], swap_sem.at[0], swap_sem.at[1], across)

    def send_ids(step, j):
        to = peer(step, j)
        return remote(pick_row, picks.at[me], id_send.at[to], id_recv.at[me], {"st": to})

    def take_ids(step, j):
        owner = peer(step, j)
        return remote(pick_row, picks.at[owner], id_send.at[owner], id_recv.at[owner], {"st": owner})

    def hand(kind, c):
        at = pl.ds(c * chunk_passages, chunk_passages)
        source, target, to = [(0, 1, 1), (0, 2, 2), (2, 2, 1)][kind]
        return remote(
            tables[source].at[at],
            tables[target].at[at],
            table_send.at[kind, c],
            table_recv.at[target - 1, c],
            {"st": beside[to]},
        )

    def wants(to, owner):
        return [wanted[to, 0, owner * capacity + r] for r in range(capacity)]

    def fill(kind):
        def body(step, j):
            to = peer(step, j)
            at = ((kind if step == 0 else 1 + step) * plane + j) * capacity
            for r, pick in enumerate(wants(to, beside[kind])):
                send_buf[at + r] = tables[kind][pick]

        return body

    def send(kind):
        def body(step, j):
            k = (kind if step == 0 else 1 + step) * plane + j
            owner = beside[kind]
            return remote(
                send_buf.at[pl.ds(k * capacity, capacity)],
                received.at[pl.ds(owner * capacity, capacity)],
                send_sem.at[k],
                recv_sem.at[owner],
                {"st": peer(step, j)},
            )

        return body

    def take(step, j):
        owner = peer(step, j)
        return remote(
            send_buf.at[pl.ds(0, capacity)],
            received.at[pl.ds(owner * capacity, capacity)],
            send_sem.at[0],
            recv_sem.at[owner],
            {"st": owner},
        )

    def serve(kind):
        every(fill(kind), (0,))
        every(lambda step, j: send(kind)(step, j).start(), (0,))
        owner = beside[kind]
        for r, pick in enumerate(wants(me, owner)):
            received[owner * capacity + r] = tables[kind][pick]

    def project(c):
        load(c).wait()
        memory = norm_rows(held[c], store_gain[...]).astype(jnp.bfloat16)
        raw = jnp.dot(memory, pair[...], preferred_element_type=jnp.float32)
        keys = [
            norm_rows(raw[:, g * head_dim : (g + 1) * head_dim], key_gain[...])
            for g in range(groups)
        ]
        done = jnp.concatenate(keys + [raw[:, groups * head_dim :]], axis=1).astype(jnp.bfloat16)
        own_table[pl.ds(c * chunk_passages, chunk_passages)] = done.reshape(
            chunk_passages, passage_rows, done.shape[1]
        )

    load(0).start()
    for side in sides[:-1]:
        side.start()
    for c in range(1, chunks):
        load(c).start()
    barrier = pltpu.get_barrier_semaphore()

    def greet(step, j):
        pl.semaphore_signal(barrier, inc=1, device_id={"st": peer(step, j)}, device_id_type=MESH)

    every(greet, steps)
    pl.semaphore_signal(barrier, inc=1, device_id=across, device_id_type=MESH)

    def hand_on(c):
        if relays:
            hand(0, c).start()

            @pl.when(middle)
            def _():
                hand(1, c).start()

    for k in range(4):
        sides[k].wait()
    for c in range(chunks):
        project(c)
        if c == 0:
            sides[4].wait()
            pl.semaphore_wait(barrier, n)
            every(lambda step, j: send_ids(step, j).start(), steps)
            sides[-1].start()
            swap_tokens.start()
        else:
            hand_on(c - 1)
    for weight in weights:
        weight.start()
    hand_on(chunks - 1)
    for side in sides[5:-1]:
        side.wait()
    every(lambda step, j: take_ids(step, j).wait_recv(), steps)
    listed = pltpu.make_async_copy(picks, wanted, side_sem.at[len(sides)])
    listed.start()
    listed.wait()
    if relays:

        @pl.when(edge)
        def _():
            every(fill(0), (2, 3))
            every(lambda step, j: send(0)(step, j).start(), (2, 3))

    serve(0)

    sides[-1].wait()
    swap_tokens.wait()
    norm_tile = largest(token_rows, (128, 64, 32, 16, 8))

    def normalize(i, carry):
        rows = pl.ds(pl.multiple_of(i * norm_tile, norm_tile), norm_tile)
        whole = jnp.concatenate([half[0, rows, :], half[1, rows, :]], axis=1)
        normed[rows, :] = norm_rows(whole, norm_gain[...]).astype(jnp.bfloat16)
        return carry

    lax.fori_loop(0, token_rows // norm_tile, normalize, 0)

    weights[0].wait()
    tile_blocks = largest(token_rows // block_rows, (4, 2, 1))
    tile_rows = tile_blocks * block_rows

    def ask(i, carry):
        rows = pl.ds(pl.multiple_of(i * tile_rows, tile_rows), tile_rows)
        raw = jnp.dot(normed[rows, :], query[...], preferred_element_type=jnp.float32)
        for g in range(groups):
            heads = []
            for h in range(repeat):
                at = (g * repeat + h) * head_dim
                scale = head_scale[g * repeat + h] * (1.0 / math.sqrt(head_dim))
                head = norm_rows(raw[:, at : at + head_dim], query_gain[...]) * scale
                heads.append(head.astype(jnp.bfloat16))
            for b in range(tile_blocks):
                rows = slice(b * block_rows, (b + 1) * block_rows)
                asked = jnp.concatenate([head[rows] for head in heads], axis=0)
                q[(i * tile_blocks + b) * groups + g] = jnp.transpose(asked)
        return carry

    lax.fori_loop(0, token_rows // tile_rows, ask, 0)

    for weight in weights[1:]:
        weight.wait()
    conv_rows = largest(token_rows // SEQ, (4, 2, 1)) * SEQ
    conv_columns = largest(conv.shape[1] // LANES, (2, 1)) * LANES
    down_tiles = token_rows // conv_rows
    conv_tiles = conv.shape[1] // conv_columns * down_tiles

    def branch(t, carry):
        c, i = t // down_tiles, lax.rem(t, down_tiles)
        rows = pl.ds(pl.multiple_of(i * conv_rows, conv_rows), conv_rows)
        columns = pl.ds(pl.multiple_of(c * conv_columns, conv_columns), conv_columns)
        left = normed[rows, :]
        z = jnp.dot(left, gate[:, columns], preferred_element_type=jnp.float32)
        z = z * jnp.dot(left, inp[:, columns], preferred_element_type=jnp.float32)
        at = lax.rem(lax.broadcasted_iota(jnp.int32, (conv_rows, 1), 0), SEQ)
        one = jnp.where(at < 1, 0.0, pltpu.roll(z, 1, 0))
        two = jnp.where(at < 2, 0.0, pltpu.roll(z, 2, 0))
        summed = (
            two * taps[0:1, columns] + one * taps[1:2, columns] + z * taps[2:3, columns]
        )
        conv[rows, columns] = (
            jnp.dot(left, outer[:, columns], preferred_element_type=jnp.float32) * summed
        )
        return carry

    if relays:

        @pl.when(middle)
        def _():
            for c in range(chunks):
                hand(1, c).wait_recv()
                hand(2, c).start()
            for c in range(chunks):
                hand(0, c).wait_recv()
            serve(1)
            serve(2)

        first, second = conv_tiles * FIRST // 8, conv_tiles * SECOND // 8
        lax.fori_loop(0, first, branch, 0)

        @pl.when(edge)
        def _():
            for c in range(chunks):
                hand(0, c).wait_recv()
            serve(1)

        lax.fori_loop(first, second, branch, 0)

        @pl.when(edge)
        def _():
            for c in range(chunks):
                hand(2, c).wait_recv()
            serve(2)

        lax.fori_loop(second, conv_tiles, branch, 0)
    else:
        lax.fori_loop(0, conv_tiles, branch, 0)

    def attend(step, j):
        owner = peer(step, j)
        if step == 3:
            take(step, j).wait_recv()
        else:

            @pl.when(j > 0)
            def _():
                take(step, j).wait_recv()

        at = [owner * capacity + r for r in range(capacity)]
        for g in range(groups):
            key = slice(g * head_dim, (g + 1) * head_dim)
            value = slice((groups + g) * head_dim, (groups + g + 1) * head_dim)
            asked = [q[blocks[slot] * groups + g] for slot in at]
            scores = [
                lax.dot_general(
                    received[slot][:, key], ask, NN, preferred_element_type=jnp.float32
                )
                for slot, ask in zip(at, asked)
            ]
            tops = [jnp.max(score, axis=0, keepdims=True) for score in scores]
            raised = [jnp.exp(score - top) for score, top in zip(scores, tops)]
            totals = [jnp.sum(weight, axis=0, keepdims=True) for weight in raised]
            shares = [
                (weight * (1.0 / total)).astype(jnp.bfloat16)
                for weight, total in zip(raised, totals)
            ]
            parts = [
                lax.dot_general(
                    received[slot][:, value], share, TN, preferred_element_type=jnp.float32
                )
                for slot, share in zip(at, shares)
            ]
            for slot, part, top, total in zip(at, parts, tops, totals):
                partials[slot * groups + g] = part.astype(jnp.bfloat16)
                stats[slot * groups + g, 0:1, :] = top
                stats[slot * groups + g, 1:2, :] = total

    every(attend, steps, own=True)

    block_count = token_rows // block_rows
    parts = part_send.shape[0]
    part_blocks = block_count // parts
    part_rows = part_blocks * block_rows

    own_width = attended.shape[1] // 2
    own_columns = pl.multiple_of(core * own_width, own_width)

    def swap_part(k):
        here = attended.at[pl.ds(k * part_rows, part_rows), pl.ds(own_columns, own_width)]
        return remote(here, here, part_send.at[k], part_recv.at[k], across)

    def combine(b, carry):
        for g in range(groups):
            at = [slots[p * block_count + b] * groups + g for p in range(per_block)]
            tops = [stats[s, 0:1, :] for s in at]
            highest = functools.reduce(jnp.maximum, tops)
            scales = [jnp.exp(top - highest) * stats[s, 1:2, :] for top, s in zip(tops, at)]
            denominator = functools.reduce(jnp.add, scales)
            summed = functools.reduce(
                jnp.add, [partials[s].astype(jnp.float32) * scale for s, scale in zip(at, scales)]
            )
            done = jnp.transpose(summed * (1.0 / denominator)).astype(jnp.bfloat16)
            rows = pl.ds(pl.multiple_of(b * block_rows, block_rows), block_rows)
            for h in range(repeat):
                columns = pl.ds(own_columns + (g * repeat + h) * head_dim, head_dim)
                attended[rows, columns] = done[h * block_rows : (h + 1) * block_rows]
        return carry

    for k in range(parts):
        lax.fori_loop(k * part_blocks, (k + 1) * part_blocks, combine, 0)
        if k > 0:
            swap_part(k - 1).start()
    swap_part(parts - 1).start()

    def leave(k):
        rows = pl.ds(k * part_rows, part_rows)
        return pltpu.make_async_copy(
            normed.at[rows, pl.ds(0, conv.shape[1])], mixed_hbm.at[rows], out_sem.at[k]
        )

    for i in range(down_tiles):
        mine = range(i * parts // down_tiles, (i + 1) * parts // down_tiles)
        for k in mine:
            swap_part(k).wait_recv()
        rows = pl.ds(i * conv_rows, conv_rows)

        def project_out(c, carry, rows=rows):
            columns = pl.ds(pl.multiple_of(c * conv_columns, conv_columns), conv_columns)
            cross = jnp.dot(
                attended[rows, :], out_weight[:, columns], preferred_element_type=jnp.float32
            )
            gated = jax.nn.sigmoid(gate_logit[:, columns]) * cross
            normed[rows, columns] = (conv[rows, columns] + gated).astype(jnp.bfloat16)
            return carry

        lax.fori_loop(0, conv.shape[1] // conv_columns, project_out, 0)
        for k in mine:
            leave(k).start()
    every(lambda step, j: send_ids(step, j).wait_send(), steps)
    every(lambda step, j: send(0)(step, j).wait_send(), (0,))
    if relays:
        every(lambda step, j: send(1)(step, j).wait_send(), (0,))
        every(lambda step, j: send(2)(step, j).wait_send(), (0,))
        for c in range(chunks):
            hand(0, c).wait_send()

        @pl.when(middle)
        def _():
            for c in range(chunks):
                hand(1, c).wait_send()
                hand(2, c).wait_send()

        @pl.when(edge)
        def _():
            every(lambda step, j: send(0)(step, j).wait_send(), (2, 3))

    for k in range(parts):
        swap_part(k).wait_send()
        leave(k).wait()


def on_device(
    planes,
    tokens,
    norm_gain,
    branch_outer,
    branch_gate,
    branch_input,
    conv_taps,
    query_weight,
    query_gain,
    head_scale,
    store,
    store_gain,
    key_weight,
    value_weight,
    key_gain,
    out_weight,
    gate_logit,
    passage_ids,
):
    n = lax.axis_size("st")
    token_rows, local_width = tokens.shape
    head_dim = query_gain.shape[0]
    local_heads = query_weight.shape[1] // head_dim
    groups = key_weight.shape[1] // head_dim
    repeat = local_heads // groups
    block_count, per_block = passage_ids.shape
    block_rows = token_rows // block_count
    passages, passage_rows, width = store.shape
    channels = branch_outer.shape[1]
    requests = block_count * per_block
    capacity = max(2, (requests + n - 1) // n)
    count = n * capacity
    flat = passage_ids.T.reshape(requests)
    owners = flat // passages
    order = jnp.arange(requests, dtype=jnp.int32)
    earlier = (owners[:, None] == owners[None, :]) & (order[None, :] < order[:, None])
    slots = owners * capacity + jnp.sum(earlier.astype(jnp.int32), axis=1)
    lanes = LANES * ((count + LANES - 1) // LANES)
    filled = slots[None, :] == jnp.arange(lanes, dtype=jnp.int32)[:, None]
    pick = jnp.sum(jnp.where(filled, (flat - owners * passages)[None], 0), axis=1)
    blocks = jnp.sum(jnp.where(filled, lax.rem(order, block_count)[None], 0), axis=1)

    rows = passages * passage_rows
    chunks = largest(passages, (4, 2, 1))
    parts = largest(block_count, (4, 2, 1))
    pair_width = key_weight.shape[1] + value_weight.shape[1]
    wide = repeat * block_rows
    plane = n // planes
    relays = planes == 4
    buffers = 5 * plane if relays else plane
    bf16, f32 = jnp.bfloat16, jnp.float32
    dma = pltpu.SemaphoreType.DMA
    smem = pl.BlockSpec(memory_space=pltpu.SMEM)
    anywhere = pl.BlockSpec(memory_space=pl.ANY)
    cfg = (n, planes, capacity, per_block, groups, repeat, head_dim, block_rows)
    return pl.pallas_call(
        functools.partial(layer_kernel, cfg),
        out_shape=jax.ShapeDtypeStruct((token_rows, channels), bf16),
        in_specs=[smem] * 3 + [anywhere] * 16,
        out_specs=anywhere,
        scratch_shapes=[
            pltpu.VMEM((2, token_rows, local_width), bf16),
            pltpu.VMEM((token_rows, width), bf16),
            pltpu.VMEM((width, channels), bf16),
            pltpu.VMEM((width, channels), bf16),
            pltpu.VMEM((width, channels), bf16),
            pltpu.VMEM(query_weight.shape, bf16),
            pltpu.VMEM(out_weight.shape, bf16),
            pltpu.VMEM((width, pair_width), bf16),
            pltpu.VMEM((chunks, rows // chunks, width), bf16),
            pltpu.VMEM((passages, passage_rows, pair_width), bf16),
            pltpu.VMEM((passages if relays else 1, passage_rows, pair_width), bf16),
            pltpu.VMEM((passages if relays else 1, passage_rows, pair_width), bf16),
            pltpu.VMEM((buffers * capacity, passage_rows, pair_width), bf16),
            pltpu.VMEM((count, passage_rows, pair_width), bf16),
            pltpu.VMEM((block_count * groups, head_dim, wide), bf16),
            pltpu.VMEM((count * groups, head_dim, wide), bf16),
            pltpu.VMEM((count * groups, 2, wide), f32),
            pltpu.VMEM((token_rows, 2 * local_heads * head_dim), bf16),
            pltpu.VMEM((token_rows, channels), f32),
            pltpu.VMEM((1, width), f32),
            pltpu.VMEM(conv_taps.shape, f32),
            pltpu.VMEM((1, head_dim), f32),
            pltpu.VMEM((1, width), f32),
            pltpu.VMEM((1, head_dim), f32),
            pltpu.VMEM((1, channels), f32),
            pltpu.VMEM((1, lanes), jnp.int32),
            pltpu.VMEM((n, 1, lanes), jnp.int32),
            pltpu.SMEM((n, 1, lanes), jnp.int32),
            dma((chunks,)),
            dma((12,)),
            dma((5,)),
            dma((2,)),
            dma((n,)),
            dma((n,)),
            dma((3, chunks)),
            dma((2, chunks)),
            dma((buffers,)),
            dma((n,)),
            dma((parts,)),
            dma((parts,)),
            dma((parts,)),
        ],
        compiler_params=pltpu.CompilerParams(
            collective_id=0, has_side_effects=True, vmem_limit_bytes=62 * 1024 * 1024
        ),
        cost_estimate=pl.CostEstimate(
            flops=2 * token_rows * width * (3 * channels + local_heads * head_dim),
            bytes_accessed=8 * width * channels,
            transcendentals=0,
        ),
        name="layer",
    )(
        slots,
        blocks,
        head_scale,
        pick[None],
        tokens,
        norm_gain[None],
        branch_outer,
        branch_gate,
        branch_input,
        conv_taps,
        query_weight,
        query_gain[None],
        store.reshape(rows, width),
        store_gain[None],
        key_weight,
        value_weight,
        key_gain[None],
        out_weight,
        gate_logit[None],
    )


FIRST, SECOND = 2, 6


def planes_of(mesh):
    line = mesh.devices.reshape(mesh.shape["st"], -1)[:, 0]
    heights = [getattr(d, "coords", (0, 0, 0))[2] for d in line]
    planes = len(set(heights))
    plane = len(heights) // planes
    ordered = heights == [h for h in sorted(set(heights)) for _ in range(plane)]
    return planes if planes == 4 and ordered else 1


def solution(mesh):
    return jax.shard_map(
        functools.partial(on_device, planes_of(mesh)),
        mesh=mesh,
        in_specs=(
            P("st", "tp"),
            P(),
            P(None, "tp"),
            P(None, "tp"),
            P(None, "tp"),
            P(None, "tp"),
            P(None, "tp"),
            P(),
            P("tp"),
            P("st", None, None),
            P(),
            P(None, "tp"),
            P(None, "tp"),
            P(),
            P(None, "tp"),
            P("tp"),
            P("st", None),
        ),
        out_specs=P("st", "tp"),
        check_vma=False,
    )
```

```python
import functools
import math

import jax
import jax.numpy as jnp
from jax import lax
from jax.experimental import pallas as pl
from jax.experimental.pallas import tpu as pltpu
from jax.sharding import PartitionSpec as P

MESH = pl.DeviceIdType.MESH
LANES = 128
SEQ = 128
EPS = 1e-06
NN = (((1,), (0,)), ((), ()))
TN = (((0,), (0,)), ((), ()))


def norm_rows(values, gain):
    values = values.astype(jnp.float32)
    return values * lax.rsqrt(jnp.mean(values * values, axis=-1, keepdims=True) + EPS) * gain


def largest(total, options):
    return next(c for c in options if total % c == 0)


def layer_kernel(
    cfg, slots, blocks, head_scale, pick_hbm, tokens_hbm, norm_gain_hbm, outer_hbm, gate_hbm,
    input_hbm, taps_hbm, query_hbm, query_gain_hbm, store_hbm, store_gain_hbm, key_hbm, value_hbm,
    key_gain_hbm, out_weight_hbm, gate_logit_hbm,
    mixed_hbm,
    half, normed, outer, gate, inp, query, out_weight, pair, held, own_table, side_table, next_table,
    send_buf, received, q, partials, stats, attended, conv, norm_gain, taps, query_gain, store_gain, key_gain,
    gate_logit, pick_row, picks, wanted,
    store_sem, side_sem, weight_sem, swap_sem, id_send, id_recv, table_send, table_recv,
    send_sem, recv_sem, part_send, part_recv, out_sem,
):
    n, planes, capacity, per_block, groups, repeat, head_dim, block_rows = cfg
    me = lax.axis_index("st")
    core = lax.axis_index("tp")
    plane = n // planes
    level, place = me // plane, lax.rem(me, plane)
    relays = planes == 4
    middle = (level == 1) | (level == 2)
    edge = jnp.logical_not(middle)
    levels = [level]
    if relays:
        half_up = level // 2
        levels += [level + 1 - 2 * lax.rem(level, 2), 2 - half_up, 3 - 3 * half_up]
    beside = [at * plane + place for at in levels]

    def peer(step, j):
        return levels[step] * plane + lax.rem(place + j, plane)

    def every(body, steps, own=False):
        for step in steps:

            def run(j, carry, step=step):
                body(step, j)
                return carry

            lax.fori_loop(1 if step == 0 and not own else 0, plane, run, 0)

    steps = tuple(range(len(levels)))
    tables = [own_table, side_table, next_table]

    chunks, chunk_rows = held.shape[0], held.shape[1]
    passage_rows = own_table.shape[1]
    chunk_passages = chunk_rows // passage_rows
    key_width = key_hbm.shape[1]
    token_rows = tokens_hbm.shape[0]

    def load(c):
        return pltpu.make_async_copy(
            store_hbm.at[pl.ds(c * chunk_rows, chunk_rows)], held.at[c], store_sem.at[c]
        )

    sides = [
        pltpu.make_async_copy(source, target, side_sem.at[k])
        for k, (source, target) in enumerate(
            [
                (store_gain_hbm, store_gain),
                (key_hbm, pair.at[:, pl.ds(0, key_width)]),
                (value_hbm, pair.at[:, pl.ds(key_width, value_hbm.shape[1])]),
                (key_gain_hbm, key_gain),
                (pick_hbm, pick_row),
                (pick_hbm, picks.at[me]),
                (norm_gain_hbm, norm_gain),
                (query_gain_hbm, query_gain),
                (taps_hbm, taps),
                (gate_logit_hbm, gate_logit),
                (tokens_hbm, half.at[core]),
            ]
        )
    ]
    weights = [
        pltpu.make_async_copy(source, target, weight_sem.at[k])
        for k, (source, target) in enumerate(
            [
                (query_hbm, query),
                (gate_hbm, gate),
                (input_hbm, inp),
                (outer_hbm, outer),
                (out_weight_hbm, out_weight),
            ]
        )
    ]

    def remote(source, target, sent, got, to):
        return pltpu.make_async_remote_copy(
            src_ref=source,
            dst_ref=target,
            send_sem=sent,
            recv_sem=got,
            device_id=to,
            device_id_type=MESH,
        )

    across = {"tp": 1 - core}
    swap_tokens = remote(tokens_hbm, half.at[core], swap_sem.at[0], swap_sem.at[1], across)

    def send_ids(step, j):
        to = peer(step, j)
        return remote(pick_row, picks.at[me], id_send.at[to], id_recv.at[me], {"st": to})

    def take_ids(step, j):
        owner = peer(step, j)
        return remote(pick_row, picks.at[owner], id_send.at[owner], id_recv.at[owner], {"st": owner})

    def hand(kind, c):
        at = pl.ds(c * chunk_passages, chunk_passages)
        source, target, to = [(0, 1, 1), (0, 2, 2), (2, 2, 1)][kind]
        return remote(
            tables[source].at[at],
            tables[target].at[at],
            table_send.at[kind, c],
            table_recv.at[target - 1, c],
            {"st": beside[to]},
        )

    def wants(to, owner):
        return [wanted[to, 0, owner * capacity + r] for r in range(capacity)]

    def fill(kind):
        def body(step, j):
            to = peer(step, j)
            at = ((kind if step == 0 else 1 + step) * plane + j) * capacity
            for r, pick in enumerate(wants(to, beside[kind])):
                send_buf[at + r] = tables[kind][pick]

        return body

    def send(kind):
        def body(step, j):
            k = (kind if step == 0 else 1 + step) * plane + j
            owner = beside[kind]
            return remote(
                send_buf.at[pl.ds(k * capacity, capacity)],
                received.at[pl.ds(owner * capacity, capacity)],
                send_sem.at[k],
                recv_sem.at[owner],
                {"st": peer(step, j)},
            )

        return body

    def take(step, j):
        owner = peer(step, j)
        return remote(
            send_buf.at[pl.ds(0, capacity)],
            received.at[pl.ds(owner * capacity, capacity)],
            send_sem.at[0],
            recv_sem.at[owner],
            {"st": owner},
        )

    def serve(kind):
        every(fill(kind), (0,))
        every(lambda step, j: send(kind)(step, j).start(), (0,))
        owner = beside[kind]
        for r, pick in enumerate(wants(me, owner)):
            received[owner * capacity + r] = tables[kind][pick]

    def project(c):
        load(c).wait()
        memory = norm_rows(held[c], store_gain[...]).astype(jnp.bfloat16)
        raw = jnp.dot(memory, pair[...], preferred_element_type=jnp.float32)
        keys = [
            norm_rows(raw[:, g * head_dim : (g + 1) * head_dim], key_gain[...])
            for g in range(groups)
        ]
        done = jnp.concatenate(keys + [raw[:, groups * head_dim :]], axis=1).astype(jnp.bfloat16)
        own_table[pl.ds(c * chunk_passages, chunk_passages)] = done.reshape(
            chunk_passages, passage_rows, done.shape[1]
        )

    load(0).start()
    for side in sides[:-1]:
        side.start()
    for c in range(1, chunks):
        load(c).start()
    barrier = pltpu.get_barrier_semaphore()

    def greet(step, j):
        pl.semaphore_signal(barrier, inc=1, device_id={"st": peer(step, j)}, device_id_type=MESH)

    every(greet, steps)
    pl.semaphore_signal(barrier, inc=1, device_id=across, device_id_type=MESH)

    def hand_on(c):
        if relays:
            hand(0, c).start()

            @pl.when(middle)
            def _():
                hand(1, c).start()

    for k in range(4):
        sides[k].wait()
    for c in range(chunks):
        project(c)
        if c == 0:
            sides[4].wait()
            pl.semaphore_wait(barrier, n)
            every(lambda step, j: send_ids(step, j).start(), steps)
            sides[-1].start()
            swap_tokens.start()
        else:
            hand_on(c - 1)
    for weight in weights:
        weight.start()
    hand_on(chunks - 1)
    for side in sides[5:-1]:
        side.wait()
    every(lambda step, j: take_ids(step, j).wait_recv(), steps)
    listed = pltpu.make_async_copy(picks, wanted, side_sem.at[len(sides)])
    listed.start()
    listed.wait()
    serve(0)
    if relays:

        @pl.when(edge)
        def _():
            every(fill(0), (2, 3))
            every(lambda step, j: send(0)(step, j).start(), (2, 3))


    sides[-1].wait()
    swap_tokens.wait()
    norm_tile = largest(token_rows, (128, 64, 32, 16, 8))

    def normalize(i, carry):
        rows = pl.ds(pl.multiple_of(i * norm_tile, norm_tile), norm_tile)
        whole = jnp.concatenate([half[0, rows, :], half[1, rows, :]], axis=1)
        normed[rows, :] = norm_rows(whole, norm_gain[...]).astype(jnp.bfloat16)
        return carry

    lax.fori_loop(0, token_rows // norm_tile, normalize, 0)

    weights[0].wait()
    tile_blocks = largest(token_rows // block_rows, (4, 2, 1))
    tile_rows = tile_blocks * block_rows

    def ask(i, carry):
        rows = pl.ds(pl.multiple_of(i * tile_rows, tile_rows), tile_rows)
        raw = jnp.dot(normed[rows, :], query[...], preferred_element_type=jnp.float32)
        for g in range(groups):
            heads = []
            for h in range(repeat):
                at = (g * repeat + h) * head_dim
                scale = head_scale[g * repeat + h] * (1.0 / math.sqrt(head_dim))
                head = norm_rows(raw[:, at : at + head_dim], query_gain[...]) * scale
                heads.append(head.astype(jnp.bfloat16))
            for b in range(tile_blocks):
                rows = slice(b * block_rows, (b + 1) * block_rows)
                asked = jnp.concatenate([head[rows] for head in heads], axis=0)
                q[(i * tile_blocks + b) * groups + g] = jnp.transpose(asked)
        return carry

    lax.fori_loop(0, token_rows // tile_rows, ask, 0)

    for weight in weights[1:]:
        weight.wait()
    conv_rows = largest(token_rows // SEQ, (4, 2, 1)) * SEQ
    conv_columns = largest(conv.shape[1] // LANES, (2, 1)) * LANES
    down_tiles = token_rows // conv_rows
    conv_tiles = conv.shape[1] // conv_columns * down_tiles

    def branch(t, carry):
        c, i = t // down_tiles, lax.rem(t, down_tiles)
        rows = pl.ds(pl.multiple_of(i * conv_rows, conv_rows), conv_rows)
        columns = pl.ds(pl.multiple_of(c * conv_columns, conv_columns), conv_columns)
        left = normed[rows, :]
        z = jnp.dot(left, gate[:, columns], preferred_element_type=jnp.float32)
        z = z * jnp.dot(left, inp[:, columns], preferred_element_type=jnp.float32)
        at = lax.rem(lax.broadcasted_iota(jnp.int32, (conv_rows, 1), 0), SEQ)
        one = jnp.where(at < 1, 0.0, pltpu.roll(z, 1, 0))
        two = jnp.where(at < 2, 0.0, pltpu.roll(z, 2, 0))
        summed = (
            two * taps[0:1, columns] + one * taps[1:2, columns] + z * taps[2:3, columns]
        )
        conv[rows, columns] = (
            jnp.dot(left, outer[:, columns], preferred_element_type=jnp.float32) * summed
        )
        return carry

    if relays:

        @pl.when(middle)
        def _():
            for c in range(chunks):
                hand(1, c).wait_recv()
                hand(2, c).start()
            for c in range(chunks):
                hand(0, c).wait_recv()
            serve(1)
            serve(2)

        first, second = conv_tiles * FIRST // 8, conv_tiles * SECOND // 8
        lax.fori_loop(0, first, branch, 0)

        @pl.when(edge)
        def _():
            for c in range(chunks):
                hand(0, c).wait_recv()
            serve(1)

        lax.fori_loop(first, second, branch, 0)

        @pl.when(edge)
        def _():
            for c in range(chunks):
                hand(2, c).wait_recv()
            serve(2)

        lax.fori_loop(second, conv_tiles, branch, 0)
    else:
        lax.fori_loop(0, conv_tiles, branch, 0)

    def attend(step, j):
        owner = peer(step, j)
        if step == 3:
            take(step, j).wait_recv()
        else:

            @pl.when(j > 0)
            def _():
                take(step, j).wait_recv()

        at = [owner * capacity + r for r in range(capacity)]
        for g in range(groups):
            key = slice(g * head_dim, (g + 1) * head_dim)
            value = slice((groups + g) * head_dim, (groups + g + 1) * head_dim)
            asked = [q[blocks[slot] * groups + g] for slot in at]
            scores = [
                lax.dot_general(
                    received[slot][:, key], ask, NN, preferred_element_type=jnp.float32
                )
                for slot, ask in zip(at, asked)
            ]
            tops = [jnp.max(score, axis=0, keepdims=True) for score in scores]
            raised = [jnp.exp(score - top) for score, top in zip(scores, tops)]
            totals = [jnp.sum(weight, axis=0, keepdims=True) for weight in raised]
            shares = [
                (weight * (1.0 / total)).astype(jnp.bfloat16)
                for weight, total in zip(raised, totals)
            ]
            parts = [
                lax.dot_general(
                    received[slot][:, value], share, TN, preferred_element_type=jnp.float32
                )
                for slot, share in zip(at, shares)
            ]
            for slot, part, top, total in zip(at, parts, tops, totals):
                partials[slot * groups + g] = part.astype(jnp.bfloat16)
                stats[slot * groups + g, 0:1, :] = top
                stats[slot * groups + g, 1:2, :] = total

    every(attend, steps, own=True)

    block_count = token_rows // block_rows
    parts = part_send.shape[0]
    part_blocks = block_count // parts
    part_rows = part_blocks * block_rows

    own_width = attended.shape[1] // 2
    own_columns = pl.multiple_of(core * own_width, own_width)

    def swap_part(k):
        here = attended.at[pl.ds(k * part_rows, part_rows), pl.ds(own_columns, own_width)]
        return remote(here, here, part_send.at[k], part_recv.at[k], across)

    def combine(b, carry):
        for g in range(groups):
            at = [slots[p * block_count + b] * groups + g for p in range(per_block)]
            tops = [stats[s, 0:1, :] for s in at]
            highest = functools.reduce(jnp.maximum, tops)
            scales = [jnp.exp(top - highest) * stats[s, 1:2, :] for top, s in zip(tops, at)]
            denominator = functools.reduce(jnp.add, scales)
            summed = functools.reduce(
                jnp.add, [partials[s].astype(jnp.float32) * scale for s, scale in zip(at, scales)]
            )
            done = jnp.transpose(summed * (1.0 / denominator)).astype(jnp.bfloat16)
            rows = pl.ds(b * block_rows, block_rows)
            for h in range(repeat):
                columns = pl.ds(own_columns + (g * repeat + h) * head_dim, head_dim)
                attended[rows, columns] = done[h * block_rows : (h + 1) * block_rows]
        return carry

    for k in range(parts):
        for b in range(k * part_blocks, (k + 1) * part_blocks):
            combine(b, 0)
        if k > 0:
            swap_part(k - 1).start()
    swap_part(parts - 1).start()

    def leave(k):
        rows = pl.ds(k * part_rows, part_rows)
        return pltpu.make_async_copy(
            normed.at[rows, pl.ds(0, conv.shape[1])], mixed_hbm.at[rows], out_sem.at[k]
        )

    for i in range(down_tiles):
        mine = range(i * parts // down_tiles, (i + 1) * parts // down_tiles)
        for k in mine:
            swap_part(k).wait_recv()
        rows = pl.ds(i * conv_rows, conv_rows)

        def project_out(c, carry, rows=rows):
            columns = pl.ds(pl.multiple_of(c * conv_columns, conv_columns), conv_columns)
            cross = jnp.dot(
                attended[rows, :], out_weight[:, columns], preferred_element_type=jnp.float32
            )
            gated = jax.nn.sigmoid(gate_logit[:, columns]) * cross
            normed[rows, columns] = (conv[rows, columns] + gated).astype(jnp.bfloat16)
            return carry

        lax.fori_loop(0, conv.shape[1] // conv_columns, project_out, 0)
        for k in mine:
            leave(k).start()
    every(lambda step, j: send_ids(step, j).wait_send(), steps)
    every(lambda step, j: send(0)(step, j).wait_send(), (0,))
    if relays:
        every(lambda step, j: send(1)(step, j).wait_send(), (0,))
        every(lambda step, j: send(2)(step, j).wait_send(), (0,))
        for c in range(chunks):
            hand(0, c).wait_send()

        @pl.when(middle)
        def _():
            for c in range(chunks):
                hand(1, c).wait_send()
                hand(2, c).wait_send()

        @pl.when(edge)
        def _():
            every(lambda step, j: send(0)(step, j).wait_send(), (2, 3))

    for k in range(parts):
        swap_part(k).wait_send()
        leave(k).wait()


def settle_kernel(source, target, held, load_sem, store_sem):
    parts = load_sem.shape[0]
    rows = source.shape[0] // parts

    def load(k):
        at = pl.ds(k * rows, rows)
        return pltpu.make_async_copy(source.at[at], held.at[at], load_sem.at[k])

    def store(k):
        at = pl.ds(k * rows, rows)
        return pltpu.make_async_copy(held.at[at], target.at[at], store_sem.at[k])

    for k in range(parts):
        load(k).start()
    for k in range(parts):
        load(k).wait()
        store(k).start()
    for k in range(parts):
        store(k).wait()


def settle(values):
    parts = largest(values.shape[0] // 16, (8, 4, 2, 1))
    return pl.pallas_call(
        settle_kernel,
        out_shape=jax.ShapeDtypeStruct(values.shape, values.dtype),
        in_specs=[pl.BlockSpec(memory_space=pl.ANY)],
        out_specs=pl.BlockSpec(memory_space=pl.ANY),
        scratch_shapes=[
            pltpu.VMEM(values.shape, values.dtype),
            pltpu.SemaphoreType.DMA((parts,)),
            pltpu.SemaphoreType.DMA((parts,)),
        ],
        compiler_params=pltpu.CompilerParams(vmem_limit_bytes=62 * 1024 * 1024),
        name="settle",
    )(values)


def on_device(
    planes,
    tokens,
    norm_gain,
    branch_outer,
    branch_gate,
    branch_input,
    conv_taps,
    query_weight,
    query_gain,
    head_scale,
    store,
    store_gain,
    key_weight,
    value_weight,
    key_gain,
    out_weight,
    gate_logit,
    passage_ids,
):
    n = lax.axis_size("st")
    token_rows, local_width = tokens.shape
    head_dim = query_gain.shape[0]
    local_heads = query_weight.shape[1] // head_dim
    groups = key_weight.shape[1] // head_dim
    repeat = local_heads // groups
    block_count, per_block = passage_ids.shape
    block_rows = token_rows // block_count
    passages, passage_rows, width = store.shape
    channels = branch_outer.shape[1]
    requests = block_count * per_block
    capacity = max(2, (requests + n - 1) // n)
    count = n * capacity
    flat = passage_ids.T.reshape(requests)
    owners = flat // passages
    order = jnp.arange(requests, dtype=jnp.int32)
    earlier = (owners[:, None] == owners[None, :]) & (order[None, :] < order[:, None])
    slots = owners * capacity + jnp.sum(earlier.astype(jnp.int32), axis=1)
    lanes = LANES * ((count + LANES - 1) // LANES)
    filled = slots[None, :] == jnp.arange(lanes, dtype=jnp.int32)[:, None]
    pick = jnp.sum(jnp.where(filled, (flat - owners * passages)[None], 0), axis=1)
    blocks = jnp.sum(jnp.where(filled, lax.rem(order, block_count)[None], 0), axis=1)

    rows = passages * passage_rows
    chunks = largest(passages, (4, 2, 1))
    parts = largest(block_count, (4, 2, 1))
    pair_width = key_weight.shape[1] + value_weight.shape[1]
    wide = repeat * block_rows
    plane = n // planes
    relays = planes == 4
    buffers = 5 * plane if relays else plane
    bf16, f32 = jnp.bfloat16, jnp.float32
    dma = pltpu.SemaphoreType.DMA
    smem = pl.BlockSpec(memory_space=pltpu.SMEM)
    anywhere = pl.BlockSpec(memory_space=pl.ANY)
    cfg = (n, planes, capacity, per_block, groups, repeat, head_dim, block_rows)
    mixed = pl.pallas_call(
        functools.partial(layer_kernel, cfg),
        out_shape=jax.ShapeDtypeStruct((token_rows, channels), bf16),
        in_specs=[smem] * 3 + [anywhere] * 16,
        out_specs=anywhere,
        scratch_shapes=[
            pltpu.VMEM((2, token_rows, local_width), bf16),
            pltpu.VMEM((token_rows, width), bf16),
            pltpu.VMEM((width, channels), bf16),
            pltpu.VMEM((width, channels), bf16),
            pltpu.VMEM((width, channels), bf16),
            pltpu.VMEM(query_weight.shape, bf16),
            pltpu.VMEM(out_weight.shape, bf16),
            pltpu.VMEM((width, pair_width), bf16),
            pltpu.VMEM((chunks, rows // chunks, width), bf16),
            pltpu.VMEM((passages, passage_rows, pair_width), bf16),
            pltpu.VMEM((passages if relays else 1, passage_rows, pair_width), bf16),
            pltpu.VMEM((passages if relays else 1, passage_rows, pair_width), bf16),
            pltpu.VMEM((buffers * capacity, passage_rows, pair_width), bf16),
            pltpu.VMEM((count, passage_rows, pair_width), bf16),
            pltpu.VMEM((block_count * groups, head_dim, wide), bf16),
            pltpu.VMEM((count * groups, head_dim, wide), bf16),
            pltpu.VMEM((count * groups, 2, wide), f32),
            pltpu.VMEM((token_rows, 2 * local_heads * head_dim), bf16),
            pltpu.VMEM((token_rows, channels), f32),
            pltpu.VMEM((1, width), f32),
            pltpu.VMEM(conv_taps.shape, f32),
            pltpu.VMEM((1, head_dim), f32),
            pltpu.VMEM((1, width), f32),
            pltpu.VMEM((1, head_dim), f32),
            pltpu.VMEM((1, channels), f32),
            pltpu.VMEM((1, lanes), jnp.int32),
            pltpu.VMEM((n, 1, lanes), jnp.int32),
            pltpu.SMEM((n, 1, lanes), jnp.int32),
            dma((chunks,)),
            dma((12,)),
            dma((5,)),
            dma((2,)),
            dma((n,)),
            dma((n,)),
            dma((3, chunks)),
            dma((2, chunks)),
            dma((buffers,)),
            dma((n,)),
            dma((parts,)),
            dma((parts,)),
            dma((parts,)),
        ],
        compiler_params=pltpu.CompilerParams(
            collective_id=0, has_side_effects=True, vmem_limit_bytes=62 * 1024 * 1024
        ),
        cost_estimate=pl.CostEstimate(
            flops=2 * token_rows * width * (3 * channels + local_heads * head_dim),
            bytes_accessed=8 * width * channels,
            transcendentals=0,
        ),
        name="layer",
    )(
        slots,
        blocks,
        head_scale,
        pick[None],
        tokens,
        norm_gain[None],
        branch_outer,
        branch_gate,
        branch_input,
        conv_taps,
        query_weight,
        query_gain[None],
        store.reshape(rows, width),
        store_gain[None],
        key_weight,
        value_weight,
        key_gain[None],
        out_weight,
        gate_logit[None],
    )
    return settle(mixed)


FIRST, SECOND = 2, 6


def planes_of(mesh):
    line = mesh.devices.reshape(mesh.shape["st"], -1)[:, 0]
    heights = [getattr(d, "coords", (0, 0, 0))[2] for d in line]
    planes = len(set(heights))
    plane = len(heights) // planes
    ordered = heights == [h for h in sorted(set(heights)) for _ in range(plane)]
    return planes if planes == 4 and ordered else 1


def solution(mesh):
    return jax.shard_map(
        functools.partial(on_device, planes_of(mesh)),
        mesh=mesh,
        in_specs=(
            P("st", "tp"),
            P(),
            P(None, "tp"),
            P(None, "tp"),
            P(None, "tp"),
            P(None, "tp"),
            P(None, "tp"),
            P(),
            P("tp"),
            P("st", None, None),
            P(),
            P(None, "tp"),
            P(None, "tp"),
            P(),
            P(None, "tp"),
            P("tp"),
            P("st", None),
        ),
        out_specs=P("st", "tp"),
        check_vma=False,
    )
```

```python
import functools
import math

import jax
import jax.numpy as jnp
from jax import lax
from jax.experimental import pallas as pl
from jax.experimental.pallas import tpu as pltpu
from jax.sharding import PartitionSpec as P

MESH = pl.DeviceIdType.MESH
LANES = 128
SEQ = 128
EPS = 1e-06
NN = (((1,), (0,)), ((), ()))
TN = (((0,), (0,)), ((), ()))


def norm_rows(values, gain):
    values = values.astype(jnp.float32)
    return values * lax.rsqrt(jnp.mean(values * values, axis=-1, keepdims=True) + EPS) * gain


def largest(total, options):
    return next(c for c in options if total % c == 0)


def layer_kernel(
    cfg, slots, blocks, head_scale, pick_hbm, tokens_hbm, norm_gain_hbm, outer_hbm, gate_hbm,
    input_hbm, taps_hbm, query_hbm, query_gain_hbm, store_hbm, store_gain_hbm, key_hbm, value_hbm,
    key_gain_hbm, out_weight_hbm, gate_logit_hbm,
    mixed_hbm,
    half, normed, outer, gate, inp, query, out_weight, pair, held, own_table, side_table, next_table,
    send_buf, received, q, partials, stats, attended, conv, norm_gain, taps, query_gain, store_gain, key_gain,
    gate_logit, pick_row, picks, wanted,
    store_sem, side_sem, weight_sem, swap_sem, id_send, id_recv, table_send, table_recv,
    send_sem, recv_sem, part_send, part_recv, out_sem,
):
    n, planes, capacity, per_block, groups, repeat, head_dim, block_rows = cfg
    me = lax.axis_index("st")
    core = lax.axis_index("tp")
    plane = n // planes
    level, place = me // plane, lax.rem(me, plane)
    relays = planes == 4
    middle = (level == 1) | (level == 2)
    edge = jnp.logical_not(middle)
    levels = [level]
    if relays:
        half_up = level // 2
        levels += [level + 1 - 2 * lax.rem(level, 2), 2 - half_up, 3 - 3 * half_up]
    beside = [at * plane + place for at in levels]

    def peer(step, j):
        return levels[step] * plane + lax.rem(place + j, plane)

    def every(body, steps, own=False):
        for step in steps:

            def run(j, carry, step=step):
                body(step, j)
                return carry

            lax.fori_loop(1 if step == 0 and not own else 0, plane, run, 0)

    steps = tuple(range(len(levels)))
    tables = [own_table, side_table, next_table]

    chunks, chunk_rows = held.shape[0], held.shape[1]
    passage_rows = own_table.shape[1]
    chunk_passages = chunk_rows // passage_rows
    key_width = key_hbm.shape[1]
    token_rows = tokens_hbm.shape[0]

    def load(c):
        return pltpu.make_async_copy(
            store_hbm.at[pl.ds(c * chunk_rows, chunk_rows)], held.at[c], store_sem.at[c]
        )

    sides = [
        pltpu.make_async_copy(source, target, side_sem.at[k])
        for k, (source, target) in enumerate(
            [
                (store_gain_hbm, store_gain),
                (key_hbm, pair.at[:, pl.ds(0, key_width)]),
                (value_hbm, pair.at[:, pl.ds(key_width, value_hbm.shape[1])]),
                (key_gain_hbm, key_gain),
                (pick_hbm, pick_row),
                (pick_hbm, picks.at[me]),
                (norm_gain_hbm, norm_gain),
                (query_gain_hbm, query_gain),
                (taps_hbm, taps),
                (gate_logit_hbm, gate_logit),
                (tokens_hbm, half.at[core]),
            ]
        )
    ]
    weights = [
        pltpu.make_async_copy(source, target, weight_sem.at[k])
        for k, (source, target) in enumerate(
            [
                (query_hbm, query),
                (gate_hbm, gate),
                (input_hbm, inp),
                (outer_hbm, outer),
                (out_weight_hbm, out_weight),
            ]
        )
    ]

    def remote(source, target, sent, got, to):
        return pltpu.make_async_remote_copy(
            src_ref=source,
            dst_ref=target,
            send_sem=sent,
            recv_sem=got,
            device_id=to,
            device_id_type=MESH,
        )

    across = {"tp": 1 - core}
    swap_tokens = remote(tokens_hbm, half.at[core], swap_sem.at[0], swap_sem.at[1], across)

    def send_ids(step, j):
        to = peer(step, j)
        return remote(pick_row, picks.at[me], id_send.at[to], id_recv.at[me], {"st": to})

    def take_ids(step, j):
        owner = peer(step, j)
        return remote(pick_row, picks.at[owner], id_send.at[owner], id_recv.at[owner], {"st": owner})

    def hand(kind, c):
        at = pl.ds(c * chunk_passages, chunk_passages)
        source, target, to = [(0, 1, 1), (0, 2, 2), (2, 2, 1)][kind]
        return remote(
            tables[source].at[at],
            tables[target].at[at],
            table_send.at[kind, c],
            table_recv.at[target - 1, c],
            {"st": beside[to]},
        )

    def wants(to, owner):
        return [wanted[to, 0, owner * capacity + r] for r in range(capacity)]

    def fill(kind):
        def body(step, j):
            to = peer(step, j)
            at = ((kind if step == 0 else 1 + step) * plane + j) * capacity
            for r, pick in enumerate(wants(to, beside[kind])):
                send_buf[at + r] = tables[kind][pick]

        return body

    def send(kind):
        def body(step, j):
            k = (kind if step == 0 else 1 + step) * plane + j
            owner = beside[kind]
            return remote(
                send_buf.at[pl.ds(k * capacity, capacity)],
                received.at[pl.ds(owner * capacity, capacity)],
                send_sem.at[k],
                recv_sem.at[owner],
                {"st": peer(step, j)},
            )

        return body

    def take(step, j):
        owner = peer(step, j)
        return remote(
            send_buf.at[pl.ds(0, capacity)],
            received.at[pl.ds(owner * capacity, capacity)],
            send_sem.at[0],
            recv_sem.at[owner],
            {"st": owner},
        )

    def serve(kind):
        every(fill(kind), (0,))
        every(lambda step, j: send(kind)(step, j).start(), (0,))
        owner = beside[kind]
        for r, pick in enumerate(wants(me, owner)):
            received[owner * capacity + r] = tables[kind][pick]

    def project(c):
        load(c).wait()
        memory = norm_rows(held[c], store_gain[...]).astype(jnp.bfloat16)
        raw = jnp.dot(memory, pair[...], preferred_element_type=jnp.float32)
        keys = [
            norm_rows(raw[:, g * head_dim : (g + 1) * head_dim], key_gain[...])
            for g in range(groups)
        ]
        done = jnp.concatenate(keys + [raw[:, groups * head_dim :]], axis=1).astype(jnp.bfloat16)
        own_table[pl.ds(c * chunk_passages, chunk_passages)] = done.reshape(
            chunk_passages, passage_rows, done.shape[1]
        )

    load(0).start()
    for side in sides[:-1]:
        side.start()
    for c in range(1, chunks):
        load(c).start()
    barrier = pltpu.get_barrier_semaphore()

    def greet(step, j):
        pl.semaphore_signal(barrier, inc=1, device_id={"st": peer(step, j)}, device_id_type=MESH)

    every(greet, steps)
    pl.semaphore_signal(barrier, inc=1, device_id=across, device_id_type=MESH)

    def hand_on(c):
        if relays:
            hand(0, c).start()

            @pl.when(middle)
            def _():
                hand(1, c).start()

    for k in range(4):
        sides[k].wait()
    for c in range(chunks):
        project(c)
        if c == 0:
            sides[4].wait()
            pl.semaphore_wait(barrier, n)
            every(lambda step, j: send_ids(step, j).start(), steps)
            sides[-1].start()
            swap_tokens.start()
        else:
            hand_on(c - 1)
    for weight in weights:
        weight.start()
    hand_on(chunks - 1)
    for side in sides[5:-1]:
        side.wait()
    every(lambda step, j: take_ids(step, j).wait_recv(), steps)
    listed = pltpu.make_async_copy(picks, wanted, side_sem.at[len(sides)])
    listed.start()
    listed.wait()
    serve(0)
    if relays:

        @pl.when(edge)
        def _():
            every(fill(0), (2, 3))
            every(lambda step, j: send(0)(step, j).start(), (2, 3))


    sides[-1].wait()
    swap_tokens.wait()
    norm_tile = largest(token_rows, (128, 64, 32, 16, 8))

    def normalize(i, carry):
        rows = pl.ds(pl.multiple_of(i * norm_tile, norm_tile), norm_tile)
        whole = jnp.concatenate([half[0, rows, :], half[1, rows, :]], axis=1)
        normed[rows, :] = norm_rows(whole, norm_gain[...]).astype(jnp.bfloat16)
        return carry

    lax.fori_loop(0, token_rows // norm_tile, normalize, 0)

    weights[0].wait()
    tile_blocks = largest(token_rows // block_rows, (4, 2, 1))
    tile_rows = tile_blocks * block_rows

    def ask(i, carry):
        rows = pl.ds(pl.multiple_of(i * tile_rows, tile_rows), tile_rows)
        raw = jnp.dot(normed[rows, :], query[...], preferred_element_type=jnp.float32)
        for g in range(groups):
            heads = []
            for h in range(repeat):
                at = (g * repeat + h) * head_dim
                scale = head_scale[g * repeat + h] * (1.0 / math.sqrt(head_dim))
                head = norm_rows(raw[:, at : at + head_dim], query_gain[...]) * scale
                heads.append(head.astype(jnp.bfloat16))
            for b in range(tile_blocks):
                rows = slice(b * block_rows, (b + 1) * block_rows)
                asked = jnp.concatenate([head[rows] for head in heads], axis=0)
                q[(i * tile_blocks + b) * groups + g] = jnp.transpose(asked)
        return carry

    lax.fori_loop(0, token_rows // tile_rows, ask, 0)

    for weight in weights[1:]:
        weight.wait()
    conv_rows = largest(token_rows // SEQ, (4, 2, 1)) * SEQ
    conv_columns = largest(conv.shape[1] // LANES, (2, 1)) * LANES
    down_tiles = token_rows // conv_rows
    conv_tiles = conv.shape[1] // conv_columns * down_tiles

    def branch(t, carry):
        c, i = t // down_tiles, lax.rem(t, down_tiles)
        rows = pl.ds(pl.multiple_of(i * conv_rows, conv_rows), conv_rows)
        columns = pl.ds(pl.multiple_of(c * conv_columns, conv_columns), conv_columns)
        left = normed[rows, :]
        z = jnp.dot(left, gate[:, columns], preferred_element_type=jnp.float32)
        z = z * jnp.dot(left, inp[:, columns], preferred_element_type=jnp.float32)
        at = lax.rem(lax.broadcasted_iota(jnp.int32, (conv_rows, 1), 0), SEQ)
        one = jnp.where(at < 1, 0.0, pltpu.roll(z, 1, 0))
        two = jnp.where(at < 2, 0.0, pltpu.roll(z, 2, 0))
        summed = (
            two * taps[0:1, columns] + one * taps[1:2, columns] + z * taps[2:3, columns]
        )
        conv[rows, columns] = (
            jnp.dot(left, outer[:, columns], preferred_element_type=jnp.float32) * summed
        )
        return carry

    if relays:

        @pl.when(middle)
        def _():
            for c in range(chunks):
                hand(1, c).wait_recv()
                hand(2, c).start()
            for c in range(chunks):
                hand(0, c).wait_recv()
            serve(1)
            serve(2)

        first, second = conv_tiles * FIRST // 8, conv_tiles * SECOND // 8
        lax.fori_loop(0, first, branch, 0)

        @pl.when(edge)
        def _():
            for c in range(chunks):
                hand(0, c).wait_recv()
            serve(1)

        lax.fori_loop(first, second, branch, 0)

        @pl.when(edge)
        def _():
            for c in range(chunks):
                hand(2, c).wait_recv()
            serve(2)

        lax.fori_loop(second, conv_tiles, branch, 0)
    else:
        lax.fori_loop(0, conv_tiles, branch, 0)

    def attend(step, j):
        owner = peer(step, j)
        if step == 3:
            take(step, j).wait_recv()
        else:

            @pl.when(j > 0)
            def _():
                take(step, j).wait_recv()

        at = [owner * capacity + r for r in range(capacity)]
        for g in range(groups):
            key = slice(g * head_dim, (g + 1) * head_dim)
            value = slice((groups + g) * head_dim, (groups + g + 1) * head_dim)
            asked = [q[blocks[slot] * groups + g] for slot in at]
            scores = [
                lax.dot_general(
                    received[slot][:, key], ask, NN, preferred_element_type=jnp.float32
                )
                for slot, ask in zip(at, asked)
            ]
            tops = [jnp.max(score, axis=0, keepdims=True) for score in scores]
            raised = [jnp.exp(score - top) for score, top in zip(scores, tops)]
            totals = [jnp.sum(weight, axis=0, keepdims=True) for weight in raised]
            shares = [
                (weight * (1.0 / total)).astype(jnp.bfloat16)
                for weight, total in zip(raised, totals)
            ]
            parts = [
                lax.dot_general(
                    received[slot][:, value], share, TN, preferred_element_type=jnp.float32
                )
                for slot, share in zip(at, shares)
            ]
            for slot, part, top, total in zip(at, parts, tops, totals):
                partials[slot * groups + g] = part.astype(jnp.bfloat16)
                stats[slot * groups + g, 0:1, :] = top
                stats[slot * groups + g, 1:2, :] = total

    every(attend, steps, own=True)

    block_count = token_rows // block_rows
    parts = part_send.shape[0]
    part_blocks = block_count // parts
    part_rows = part_blocks * block_rows

    own_width = attended.shape[1] // 2
    own_columns = pl.multiple_of(core * own_width, own_width)

    def swap_part(k):
        here = attended.at[pl.ds(k * part_rows, part_rows), pl.ds(own_columns, own_width)]
        return remote(here, here, part_send.at[k], part_recv.at[k], across)

    def combine(b, carry):
        for g in range(groups):
            at = [slots[p * block_count + b] * groups + g for p in range(per_block)]
            tops = [stats[s, 0:1, :] for s in at]
            highest = functools.reduce(jnp.maximum, tops)
            scales = [jnp.exp(top - highest) * stats[s, 1:2, :] for top, s in zip(tops, at)]
            denominator = functools.reduce(jnp.add, scales)
            summed = functools.reduce(
                jnp.add, [partials[s].astype(jnp.float32) * scale for s, scale in zip(at, scales)]
            )
            done = jnp.transpose(summed * (1.0 / denominator)).astype(jnp.bfloat16)
            rows = pl.ds(b * block_rows, block_rows)
            for h in range(repeat):
                columns = pl.ds(own_columns + (g * repeat + h) * head_dim, head_dim)
                attended[rows, columns] = done[h * block_rows : (h + 1) * block_rows]
        return carry

    for k in range(parts):
        for b in range(k * part_blocks, (k + 1) * part_blocks):
            combine(b, 0)
        if k > 0:
            swap_part(k - 1).start()
    swap_part(parts - 1).start()

    across_tiles = conv_tiles // down_tiles

    def leave(i, c):
        rows = pl.ds(i * conv_rows, conv_rows)
        columns = pl.ds(pl.multiple_of(c * conv_columns, conv_columns), conv_columns)
        return pltpu.make_async_copy(
            normed.at[rows, columns], mixed_hbm.at[rows, columns], out_sem.at[i * across_tiles + c]
        )

    for i in range(down_tiles):
        mine = range(i * parts // down_tiles, (i + 1) * parts // down_tiles)
        for k in mine:
            swap_part(k).wait_recv()
        rows = pl.ds(i * conv_rows, conv_rows)

        def project_out(c, carry, rows=rows, i=i):
            columns = pl.ds(pl.multiple_of(c * conv_columns, conv_columns), conv_columns)
            cross = jnp.dot(
                attended[rows, :], out_weight[:, columns], preferred_element_type=jnp.float32
            )
            gated = jax.nn.sigmoid(gate_logit[:, columns]) * cross
            normed[rows, columns] = (conv[rows, columns] + gated).astype(jnp.bfloat16)
            leave(i, c).start()
            return carry

        lax.fori_loop(0, across_tiles, project_out, 0)
    every(lambda step, j: send_ids(step, j).wait_send(), steps)
    every(lambda step, j: send(0)(step, j).wait_send(), (0,))
    if relays:
        every(lambda step, j: send(1)(step, j).wait_send(), (0,))
        every(lambda step, j: send(2)(step, j).wait_send(), (0,))
        for c in range(chunks):
            hand(0, c).wait_send()

        @pl.when(middle)
        def _():
            for c in range(chunks):
                hand(1, c).wait_send()
                hand(2, c).wait_send()

        @pl.when(edge)
        def _():
            every(lambda step, j: send(0)(step, j).wait_send(), (2, 3))

    for k in range(parts):
        swap_part(k).wait_send()
    for i in range(down_tiles):
        for c in range(across_tiles):
            leave(i, c).wait()


def settle_kernel(source, target, held, load_sem, store_sem):
    parts = load_sem.shape[0]
    rows = source.shape[0] // parts

    def load(k):
        at = pl.ds(k * rows, rows)
        return pltpu.make_async_copy(source.at[at], held.at[at], load_sem.at[k])

    def store(k):
        at = pl.ds(k * rows, rows)
        return pltpu.make_async_copy(held.at[at], target.at[at], store_sem.at[k])

    for k in range(parts):
        load(k).start()
    for k in range(parts):
        load(k).wait()
        store(k).start()
    for k in range(parts):
        store(k).wait()


def settle(values):
    parts = largest(values.shape[0] // 16, (8, 4, 2, 1))
    return pl.pallas_call(
        settle_kernel,
        out_shape=jax.ShapeDtypeStruct(values.shape, values.dtype),
        in_specs=[pl.BlockSpec(memory_space=pl.ANY)],
        out_specs=pl.BlockSpec(memory_space=pl.ANY),
        scratch_shapes=[
            pltpu.VMEM(values.shape, values.dtype),
            pltpu.SemaphoreType.DMA((parts,)),
            pltpu.SemaphoreType.DMA((parts,)),
        ],
        compiler_params=pltpu.CompilerParams(vmem_limit_bytes=62 * 1024 * 1024),
        name="settle",
    )(values)


def on_device(
    planes,
    tokens,
    norm_gain,
    branch_outer,
    branch_gate,
    branch_input,
    conv_taps,
    query_weight,
    query_gain,
    head_scale,
    store,
    store_gain,
    key_weight,
    value_weight,
    key_gain,
    out_weight,
    gate_logit,
    passage_ids,
):
    n = lax.axis_size("st")
    token_rows, local_width = tokens.shape
    head_dim = query_gain.shape[0]
    local_heads = query_weight.shape[1] // head_dim
    groups = key_weight.shape[1] // head_dim
    repeat = local_heads // groups
    block_count, per_block = passage_ids.shape
    block_rows = token_rows // block_count
    passages, passage_rows, width = store.shape
    channels = branch_outer.shape[1]
    requests = block_count * per_block
    capacity = max(2, (requests + n - 1) // n)
    count = n * capacity
    flat = passage_ids.T.reshape(requests)
    owners = flat // passages
    order = jnp.arange(requests, dtype=jnp.int32)
    earlier = (owners[:, None] == owners[None, :]) & (order[None, :] < order[:, None])
    slots = owners * capacity + jnp.sum(earlier.astype(jnp.int32), axis=1)
    lanes = LANES * ((count + LANES - 1) // LANES)
    filled = slots[None, :] == jnp.arange(lanes, dtype=jnp.int32)[:, None]
    pick = jnp.sum(jnp.where(filled, (flat - owners * passages)[None], 0), axis=1)
    blocks = jnp.sum(jnp.where(filled, lax.rem(order, block_count)[None], 0), axis=1)

    rows = passages * passage_rows
    chunks = largest(passages, (4, 2, 1))
    parts = largest(block_count, (4, 2, 1))
    pair_width = key_weight.shape[1] + value_weight.shape[1]
    wide = repeat * block_rows
    tiles = (token_rows // (largest(token_rows // SEQ, (4, 2, 1)) * SEQ)) * (
        channels // (largest(channels // LANES, (2, 1)) * LANES)
    )
    plane = n // planes
    relays = planes == 4
    buffers = 5 * plane if relays else plane
    bf16, f32 = jnp.bfloat16, jnp.float32
    dma = pltpu.SemaphoreType.DMA
    smem = pl.BlockSpec(memory_space=pltpu.SMEM)
    anywhere = pl.BlockSpec(memory_space=pl.ANY)
    cfg = (n, planes, capacity, per_block, groups, repeat, head_dim, block_rows)
    mixed = pl.pallas_call(
        functools.partial(layer_kernel, cfg),
        out_shape=jax.ShapeDtypeStruct((token_rows, channels), bf16),
        in_specs=[smem] * 3 + [anywhere] * 16,
        out_specs=anywhere,
        scratch_shapes=[
            pltpu.VMEM((2, token_rows, local_width), bf16),
            pltpu.VMEM((token_rows, width), bf16),
            pltpu.VMEM((width, channels), bf16),
            pltpu.VMEM((width, channels), bf16),
            pltpu.VMEM((width, channels), bf16),
            pltpu.VMEM(query_weight.shape, bf16),
            pltpu.VMEM(out_weight.shape, bf16),
            pltpu.VMEM((width, pair_width), bf16),
            pltpu.VMEM((chunks, rows // chunks, width), bf16),
            pltpu.VMEM((passages, passage_rows, pair_width), bf16),
            pltpu.VMEM((passages if relays else 1, passage_rows, pair_width), bf16),
            pltpu.VMEM((passages if relays else 1, passage_rows, pair_width), bf16),
            pltpu.VMEM((buffers * capacity, passage_rows, pair_width), bf16),
            pltpu.VMEM((count, passage_rows, pair_width), bf16),
            pltpu.VMEM((block_count * groups, head_dim, wide), bf16),
            pltpu.VMEM((count * groups, head_dim, wide), bf16),
            pltpu.VMEM((count * groups, 2, wide), f32),
            pltpu.VMEM((token_rows, 2 * local_heads * head_dim), bf16),
            pltpu.VMEM((token_rows, channels), f32),
            pltpu.VMEM((1, width), f32),
            pltpu.VMEM(conv_taps.shape, f32),
            pltpu.VMEM((1, head_dim), f32),
            pltpu.VMEM((1, width), f32),
            pltpu.VMEM((1, head_dim), f32),
            pltpu.VMEM((1, channels), f32),
            pltpu.VMEM((1, lanes), jnp.int32),
            pltpu.VMEM((n, 1, lanes), jnp.int32),
            pltpu.SMEM((n, 1, lanes), jnp.int32),
            dma((chunks,)),
            dma((12,)),
            dma((5,)),
            dma((2,)),
            dma((n,)),
            dma((n,)),
            dma((3, chunks)),
            dma((2, chunks)),
            dma((buffers,)),
            dma((n,)),
            dma((parts,)),
            dma((parts,)),
            dma((tiles,)),
        ],
        compiler_params=pltpu.CompilerParams(
            collective_id=0, has_side_effects=True, vmem_limit_bytes=62 * 1024 * 1024
        ),
        cost_estimate=pl.CostEstimate(
            flops=2 * token_rows * width * (3 * channels + local_heads * head_dim),
            bytes_accessed=8 * width * channels,
            transcendentals=0,
        ),
        name="layer",
    )(
        slots,
        blocks,
        head_scale,
        pick[None],
        tokens,
        norm_gain[None],
        branch_outer,
        branch_gate,
        branch_input,
        conv_taps,
        query_weight,
        query_gain[None],
        store.reshape(rows, width),
        store_gain[None],
        key_weight,
        value_weight,
        key_gain[None],
        out_weight,
        gate_logit[None],
    )
    return settle(mixed)


FIRST, SECOND = 2, 6


def planes_of(mesh):
    line = mesh.devices.reshape(mesh.shape["st"], -1)[:, 0]
    heights = [getattr(d, "coords", (0, 0, 0))[2] for d in line]
    planes = len(set(heights))
    plane = len(heights) // planes
    ordered = heights == [h for h in sorted(set(heights)) for _ in range(plane)]
    return planes if planes == 4 and ordered else 1


def solution(mesh):
    return jax.shard_map(
        functools.partial(on_device, planes_of(mesh)),
        mesh=mesh,
        in_specs=(
            P("st", "tp"),
            P(),
            P(None, "tp"),
            P(None, "tp"),
            P(None, "tp"),
            P(None, "tp"),
            P(None, "tp"),
            P(),
            P("tp"),
            P("st", None, None),
            P(),
            P(None, "tp"),
            P(None, "tp"),
            P(),
            P(None, "tp"),
            P("tp"),
            P("st", None),
        ),
        out_specs=P("st", "tp"),
        check_vma=False,
    )
```
